1024 devices in a mesh: ep: 32 (over z, core), tp: 32 (over y, x).
Axes of the slice: x: 4, y: 8, z: 16, core: 2. Of those that a mesh axis runs over, the one named last changes fastest.
Arguments:
- tokens: bfloat16 [2048, 2048], P('ep', 'tp'), may hold values from -6 to 6
- gain_mix: float32 [2048], replicated, may hold values from 0.1 to 1.9
- w_in: bfloat16 [2048, 1024], P(None, 'tp'), may hold values from -0.125 to 0.125
- decay_rate: float32 [64, 64], P('tp'), may hold values from 0.05 to 3
- frequency: float32 [64, 64], P('tp'), may hold values from -3 to 3
- log_step: float32 [64], P('tp'), may hold values from -3 to 0
- input_real: float32 [64, 64, 16], P('tp'), may hold values from -1 to 1
- input_imag: float32 [64, 64, 16], P('tp'), may hold values from -1 to 1
- readout_real: float32 [64, 16, 64], P('tp'), may hold values from -0.75 to 0.75
- readout_imaginary: float32 [64, 16, 64], P('tp'), may hold values from -0.75 to 0.75
- passthrough_scale: float32 [1024], P('tp'), may hold values from -4 to 4
- state_real: float32 [2048, 64, 64], P('ep', 'tp'), may hold values from -4 to 4
- state_imag: float32 [2048, 64, 64], P('ep', 'tp'), may hold values from -4 to 4
- w_out: bfloat16 [1024, 2048], replicated, may hold values from -0.1875 to 0.1875
- gain_ffn: float32 [2048], replicated, may hold values from 0.1 to 1.9
- expert_choice: int32 [2048, 2], P('ep'), may hold values from 0 to 31, all different within a row; in each aligned block of 64 rows (0 to 63, 64 to 127, ...) at most 8 rows name the same one
- expert_weight: float32 [2048, 2], P('ep'), may hold values from 0.2 to 1
- w_gate: bfloat16 [32, 2048, 8192], P('ep', None, 'tp'), may hold values from -0.125 to 0.125
- w_up: bfloat16 [32, 2048, 8192], P('ep', None, 'tp'), may hold values from -0.125 to 0.125
- w_down: bfloat16 [32, 8192, 2048], P('ep', 'tp'), may hold values from -0.0625 to 0.0625
Outputs:
- layer_out: bfloat16 [2048, 2048], P('ep', 'tp')
- next_state_real: float32 [2048, 64, 64], P('ep', 'tp')
- next_state_imaginary: float32 [2048, 64, 64], P('ep', 'tp')
The draws below stay inside these ranges and needn't reach their ends.
Inputs may be any that keep to these rules, and one draw needn't show every extreme that they name: `expert_choice`: each row names 2 different experts; in the rows of one index of ep (aligned blocks of 64 rows) no expert is named more than 8 times, a bound that some block reaches.
All inputs are finite; a program needn't handle non-finite values.
Results may differ from the reference program's by a relative error of at most 0.017.
Values may be sent and summed in bfloat16 or wider, within the bound.
No kernel may reach another device: no remote copies, remote signals or barrier semaphores. Data moves between devices by JAX's collectives and lax.ppermute only.
A program may use at most 32 MiB of HBM per device.

```python
import math
import jax
import jax.numpy as jnp
import numpy as np
from jax import lax

D = 2048
SSM_WIDTH = 1024
CHANNELS = 16
STATE = 64
FF = 8192
TOP = 2
SEQS = 64
GROUPS = 64
EXPERTS = 32
CAP = 8
ROWS = 2048
N_EP = 32
N_TP = 32


def level_of(own_key, shape, shards, low, high):
    def one(position, shards_of):
        heights = jax.random.uniform(jax.random.fold_in(jax.random.fold_in(own_key, 6), position), (shards_of,), jnp.float32, low / len(shards), high / len(shards))
        return jnp.repeat(jnp.exp(heights), shape[position] // shards_of).reshape((-1,) + (1,) * (len(shape) - position - 1))

    level = one(*shards[0])
    for cut in shards[1:]:
        level = level * one(*cut)
    return level


def shared_out(stream_key, own, number, rows, number_of, top, reach, slope):
    ranking = jax.random.permutation(stream_key, number_of)
    heavy_load, common = shares(number_of, rows * top, reach, slope, True), shares(number_of, rows * top, reach, slope, False)
    places = jnp.arange(number_of)

    def named(tallies, offset_by):
        used = int((tallies > 0).sum())
        fixed = max(1, used // 4)
        passed = fixed + (places - fixed + offset_by * (used - fixed)) % max(1, number_of - fixed)
        return jnp.zeros((number_of,), jnp.int32).at[ranking[jnp.where(places < fixed, places, passed)]].set(jnp.asarray(tallies, jnp.int32))

    tallies = jnp.where(number % 4 == 0, named(heavy_load, number // 4), named(common, number - number // 4 - 1))
    mixed = jax.random.permutation(jax.random.fold_in(own, 3), number_of)
    donor, receiver = mixed[0:number_of // 2 * 2:2], mixed[1:number_of // 2 * 2:2]
    slack = jnp.minimum(tallies[donor] - 1, reach - tallies[receiver]) // 2
    slack = jnp.where((donor == ranking[0]) | (receiver == ranking[0]) | (tallies[receiver] == 0), 0, jnp.maximum(slack, 0))
    passed = jax.random.randint(jax.random.fold_in(own, 4), (number_of // 2,), 0, 1 << 20) % (slack + 1)
    tallies = tallies.at[donor].add(-passed).at[receiver].add(passed)
    members = jnp.searchsorted(jnp.cumsum(tallies), jnp.arange(rows * top), side="right").astype(jnp.int32)
    listing = members.reshape(top, rows).T
    listing = listing[jax.random.permutation(jax.random.fold_in(own, 1), rows)]
    offset_by = jax.random.randint(jax.random.fold_in(own, 2), (rows, 1), 0, top)
    return jnp.take_along_axis(listing, (jnp.arange(top)[None, :] + offset_by) % top, axis=1)


def shares(number_of, total, most, slope, full):
    weights = [(1 << 20) // math.isqrt(standing ** slope) + 1 for standing in range(1, number_of + 1)]
    largest = most if full else min(most, max(-(-total // number_of), total * weights[0] // sum(weights)))
    least = 1 if total - largest >= number_of - 1 else 0
    given, spare = [largest] + [least] * (number_of - 1), total - largest - least * (number_of - 1)
    while spare > 0:
        candidates = [i for i in range(1, number_of) if given[i] < largest] or [i for i in range(1, number_of) if given[i] < most]
        mass, budget = sum([weights[i] for i in candidates]), spare
        for i in candidates:
            more = min(most - given[i], max(1, budget * weights[i] // mass), spare)
            given[i] = given[i] + more
            spare = spare - more
    return np.array(given)


def normal_values(rng, shape, deviation, bound, split=(), kind=jnp.bfloat16):
    level = level_of(rng, shape, split, -0.22, 0.18) if split else 1.0
    array = jax.random.normal(rng, shape, jnp.float32) * deviation * level
    return jnp.minimum(jnp.maximum(array, -bound), bound).astype(kind)


def setup_inputs(seed: int = 0) -> dict:
    streams_of = jax.random.split(jax.random.key(seed), 21)
    tokens = normal_values(streams_of[0], (ROWS, D), 1.0, 6.0, ((0, 32), (1, 32)))
    gain_mix = jnp.clip(1.0 + 0.18 * jax.random.normal(streams_of[1], (D,), jnp.float32), 0.1, 1.9)
    w_in = normal_values(streams_of[2], (D, SSM_WIDTH), D ** -0.5, 0.125, ((1, 32),))
    decay_rate = jnp.clip(jnp.exp(math.log(3.0) - 4.0943445 * jax.random.uniform(streams_of[3], (GROUPS, STATE), jnp.float32) ** level_of(streams_of[3], (GROUPS, STATE), ((0, 32),), -0.2, 0.2)), 0.05, 3.0)
    frequency = jnp.clip(jax.random.uniform(streams_of[4], (GROUPS, STATE), jnp.float32, -3.0, 3.0) * level_of(streams_of[4], (GROUPS, STATE), ((0, 32),), -0.4, 0.0), -3.0, 3.0)
    log_step = jnp.clip(-3.0 + 3.0 * jax.random.uniform(streams_of[5], (GROUPS,), jnp.float32) ** level_of(streams_of[5], (GROUPS,), ((0, 32),), -0.2, 0.2), -3.0, 0.0)
    input_real = normal_values(streams_of[6], (GROUPS, STATE, CHANNELS), (2 * CHANNELS) ** -0.5, 1.0, ((0, 32),), jnp.float32)
    input_imag = normal_values(streams_of[7], (GROUPS, STATE, CHANNELS), (2 * CHANNELS) ** -0.5, 1.0, ((0, 32),), jnp.float32)
    readout_real = normal_values(streams_of[8], (GROUPS, CHANNELS, STATE), STATE ** -0.5, 0.75, ((0, 32),), jnp.float32)
    readout_imaginary = normal_values(streams_of[9], (GROUPS, CHANNELS, STATE), STATE ** -0.5, 0.75, ((0, 32),), jnp.float32)
    passthrough_scale = normal_values(streams_of[10], (SSM_WIDTH,), 1.0, 4.0, ((0, 32),), jnp.float32)
    state_real = normal_values(streams_of[11], (ROWS, GROUPS, STATE), 0.5, 4.0, ((0, 32), (1, 32)), jnp.float32)
    state_imag = normal_values(streams_of[12], (ROWS, GROUPS, STATE), 0.5, 4.0, ((0, 32), (1, 32)), jnp.float32)
    w_out = normal_values(streams_of[13], (SSM_WIDTH, D), SSM_WIDTH ** -0.5, 0.1875)
    gain_ffn = jnp.clip(1.0 + 0.18 * jax.random.normal(streams_of[14], (D,), jnp.float32), 0.1, 1.9)
    expert_choice_keys = jax.random.split(jax.random.fold_in(streams_of[15], 1), ROWS // SEQS)
    expert_choice_turns = jax.random.permutation(jax.random.fold_in(streams_of[15], 3), ROWS // SEQS)
    expert_choice = jax.vmap(lambda own, number: shared_out(jax.random.fold_in(streams_of[15], 2), own, number, SEQS, EXPERTS, TOP, CAP, 2))(expert_choice_keys, expert_choice_turns).reshape((ROWS, TOP))
    expert_weight = jnp.clip(0.2 + 0.8 * jax.random.uniform(streams_of[16], (ROWS, TOP), jnp.float32) ** level_of(streams_of[16], (ROWS, TOP), ((0, 32),), -0.2, 0.2), 0.2, 1.0)
    w_gate = normal_values(streams_of[17], (EXPERTS, D, FF), D ** -0.5, 0.125, ((0, 32), (2, 32)))
    w_up = normal_values(streams_of[18], (EXPERTS, D, FF), D ** -0.5, 0.125, ((0, 32), (2, 32)))
    w_down = normal_values(streams_of[19], (EXPERTS, FF, D), FF ** -0.5, 0.0625, ((0, 32), (1, 32)))
    return dict(tokens=tokens, gain_mix=gain_mix, w_in=w_in, decay_rate=decay_rate, frequency=frequency, log_step=log_step, input_real=input_real, input_imag=input_imag, readout_real=readout_real, readout_imaginary=readout_imaginary, passthrough_scale=passthrough_scale, state_real=state_real, state_imag=state_imag, w_out=w_out, gain_ffn=gain_ffn, expert_choice=expert_choice, expert_weight=expert_weight, w_gate=w_gate, w_up=w_up, w_down=w_down)


def rms_norm(values, gains):
    float_values = values.astype(jnp.float32)
    scale = lax.rsqrt(lax.optimization_barrier(jnp.mean(float_values * float_values, axis=-1, keepdims=True)) + 1e-06)
    return (float_values * scale * gains).astype(jnp.bfloat16)

def state_step(drive, real_state, imag_state, decay_rate, frequency, log_step, input_real, input_imag, readout_real, readout_imaginary, passthrough_scale):
    highest_precision = lax.Precision.HIGHEST
    count_of_groups, count_of_channels = (input_real.shape[0], input_real.shape[2])
    step = jnp.exp(log_step)[:, None]
    lam_real = -decay_rate
    magnitude = jnp.exp(lam_real * step)
    abar_real = magnitude * jnp.cos(frequency * step)
    abar_imag = magnitude * jnp.sin(frequency * step)
    denom = lam_real * lam_real + frequency * frequency
    numer = abar_real - 1.0
    factor_real = (numer * lam_real + abar_imag * frequency) / denom
    factor_imag = (abar_imag * lam_real - numer * frequency) / denom
    bbar_real = factor_real[..., None] * input_real - factor_imag[..., None] * input_imag
    bbar_imag = factor_real[..., None] * input_imag + factor_imag[..., None] * input_real
    float_values = drive.astype(jnp.float32).reshape(drive.shape[0], count_of_groups, count_of_channels)
    push_real = jnp.einsum('sgc,gpc->sgp', float_values, bbar_real, precision=highest_precision)
    push_imag = jnp.einsum('sgc,gpc->sgp', float_values, bbar_imag, precision=highest_precision)
    next_state_real = abar_real * real_state - abar_imag * imag_state + push_real
    next_state_imaginary = abar_real * imag_state + abar_imag * real_state + push_imag
    readout_matrix = jnp.einsum('jdr,dyr->jdy', next_state_real, readout_real, precision=highest_precision) - jnp.einsum('jdr,dyr->jdy', next_state_imaginary, readout_imaginary, precision=highest_precision) + passthrough_scale.reshape(count_of_groups, count_of_channels) * float_values
    mixer = jax.nn.gelu(readout_matrix.reshape(drive.shape[0], count_of_groups * count_of_channels)).astype(jnp.bfloat16)
    return (mixer, next_state_real, next_state_imaginary)

def slot_table(routes, expert_count, capacity):
    flat = routes.reshape(-1)
    onehot = (flat[:, None] == jnp.arange(expert_count, dtype=jnp.int32)[None, :]).astype(jnp.int32)
    before = jnp.cumsum(onehot, axis=0) - onehot
    slot = lax.optimization_barrier(jnp.sum(before * onehot, axis=1))
    target = flat * capacity + slot
    return (target[None, :] == jnp.arange(expert_count * capacity, dtype=jnp.int32)[:, None]).astype(jnp.bfloat16)

def reference(tokens, gain_mix, w_in, decay_rate, frequency, log_step, input_real, input_imag, readout_real, readout_imaginary, passthrough_scale, state_real, state_imag, w_out, gain_ffn, expert_choice, expert_weight, w_gate, w_up, w_down):
    normed = rms_norm(tokens, gain_mix)
    drive = jnp.dot(normed, w_in, preferred_element_type=jnp.float32).astype(jnp.bfloat16)
    mixer, next_state_real, next_state_imaginary = state_step(drive, state_real, state_imag, decay_rate, frequency, log_step, input_real, input_imag, readout_real, readout_imaginary, passthrough_scale)
    mixed = jnp.dot(mixer, w_out, preferred_element_type=jnp.float32).astype(jnp.bfloat16)
    after_mix = (tokens.astype(jnp.float32) + mixed.astype(jnp.float32)).astype(jnp.bfloat16)
    normed_ffn = rms_norm(after_mix, gain_ffn)
    group_rows = normed_ffn.reshape(N_EP, SEQS, D)
    routes = expert_choice.reshape(N_EP, SEQS, TOP)
    tables = jax.vmap(lambda block: slot_table(block, EXPERTS, CAP))(routes).astype(jnp.float32)
    repeated = jnp.repeat(group_rows, TOP, axis=1).astype(jnp.float32)
    sent = jnp.einsum('gks,gsd->gkd', tables, repeated).astype(jnp.bfloat16)
    sent = jnp.moveaxis(sent.reshape(N_EP, EXPERTS, CAP, D), 1, 0)
    slice_width = FF // N_TP

    def expert(inputs):
        arrived, gate_w, up_w, down_w = inputs
        flat = arrived.reshape(N_EP * CAP, D)
        gate = jnp.dot(flat, gate_w, preferred_element_type=jnp.float32)
        upper = jnp.dot(flat, up_w, preferred_element_type=jnp.float32)
        hidden = (jax.nn.silu(gate) * upper).astype(jnp.bfloat16)
        pieces = hidden.reshape(N_EP * CAP, N_TP, slice_width).astype(jnp.float32)
        downs = down_w.reshape(N_TP, slice_width, D).astype(jnp.float32)
        partial_value = jnp.einsum('rtf,tfd->rtd', pieces, downs).astype(jnp.bfloat16)
        partial_value = lax.optimization_barrier(partial_value)
        return lax.optimization_barrier(jnp.sum(partial_value.astype(jnp.float32), axis=1)).astype(jnp.bfloat16)
    results = lax.map(expert, (sent, w_gate, w_up, w_down))
    results = jnp.moveaxis(results.reshape(EXPERTS, N_EP, CAP, D), 1, 0).reshape(N_EP, EXPERTS * CAP, D)
    picked = jnp.einsum('gks,gkd->gsd', tables, results.astype(jnp.float32)).reshape(N_EP, SEQS, TOP, D)
    weighted = lax.optimization_barrier(jnp.sum(picked * expert_weight.reshape(N_EP, SEQS, TOP)[..., None], axis=2)).reshape(ROWS, D)
    layer_out = (after_mix.astype(jnp.float32) + weighted).astype(jnp.bfloat16)
    return (layer_out, next_state_real, next_state_imaginary)
```

```python
import functools

import jax
import jax.numpy as jnp
from jax import lax
from jax.experimental import pallas as pl
from jax.experimental.pallas import tpu as pltpu
from jax.sharding import Mesh
from jax.sharding import PartitionSpec as P

F32 = jnp.float32
BF16 = jnp.bfloat16
X_COUNT = 4
VMEM_LIMIT = 16 * 1024 * 1024


def exchange(parts, axis):
    return lax.all_to_all(parts, axis, split_axis=0, concat_axis=0, tiled=True)


def call(kernel, out_shape, *args, smem=(), scratch=(), flops=1_000_000):
    specs = [
        pl.BlockSpec(memory_space=pltpu.SMEM if i in smem else pltpu.VMEM) for i in range(len(args))
    ]
    outs = jax.tree.map(lambda _: pl.BlockSpec(memory_space=pltpu.VMEM), out_shape)
    return pl.pallas_call(
        kernel,
        out_shape=out_shape,
        in_specs=specs,
        out_specs=outs,
        scratch_shapes=list(scratch),
        cost_estimate=pl.CostEstimate(flops=flops, bytes_accessed=0, transcendentals=0),
        compiler_params=pltpu.CompilerParams(vmem_limit_bytes=VMEM_LIMIT),
    )(*args)


def lanes(shape):
    return lax.broadcasted_iota(jnp.int32, shape, len(shape) - 1)


def sublanes(shape):
    return lax.broadcasted_iota(jnp.int32, shape, len(shape) - 2)


def lane_roll(value, amount):
    return pltpu.roll(value, amount % value.shape[-1], value.ndim - 1)


def dot(a, b):
    return jnp.dot(a, b, preferred_element_type=F32)


def dot_nt(a, b):
    return lax.dot_general(a, b, (((1,), (1,)), ((), ())), preferred_element_type=F32)


def column_of(row):
    n = row.shape[-1]
    eye = sublanes((n, n)) == lanes((n, n))
    return jnp.sum(jnp.where(eye, jnp.broadcast_to(row, (n, n)), jnp.zeros((n, n), row.dtype)), axis=1, keepdims=True)


def spread_kernel(tokens_ref, out_ref):
    half = tokens_ref.shape[0] // 2
    values = tokens_ref[...].astype(F32)
    pair = jnp.concatenate([values[:half], values[half:]], axis=1).astype(BF16)
    for t in range(out_ref.shape[0]):
        out_ref[t] = pair


def mixer_kernel(
    arrived_ref,
    gain_ref,
    w_in_ref,
    decay_ref,
    freq_ref,
    log_step_ref,
    in_re_ref,
    in_im_ref,
    out_re_ref,
    out_im_ref,
    pass_ref,
    state_re_ref,
    state_im_ref,
    whole_ref,
    next_re_ref,
    next_im_ref,
    mixer_ref,
):
    groups, state = decay_ref.shape
    step = jnp.concatenate(
        [jnp.exp(jnp.full((1, state), log_step_ref[g], F32)) for g in range(groups)], axis=1
    )
    decay = jnp.concatenate([decay_ref[g : g + 1, :] for g in range(groups)], axis=1)
    freq = jnp.concatenate([freq_ref[g : g + 1, :] for g in range(groups)], axis=1)
    lam_re = -decay
    magnitude = jnp.exp(lam_re * step)
    abar_re = magnitude * jnp.cos(freq * step)
    abar_im = magnitude * jnp.sin(freq * step)
    denom = lam_re * lam_re + freq * freq
    numer = abar_re - 1.0
    factor_re = (numer * lam_re + abar_im * freq) / denom
    factor_im = (abar_im * lam_re - numer * freq) / denom

    def blocks(ref):
        rows = []
        for g in range(groups):
            zero = jnp.zeros_like(ref[g])
            rows.append(jnp.concatenate([ref[g] if k == g else zero for k in range(groups)], axis=1))
        return jnp.concatenate(rows, axis=0)

    in_re, in_im = blocks(in_re_ref), blocks(in_im_ref)
    bbar_re = factor_re * in_re - factor_im * in_im
    bbar_im = factor_re * in_im + factor_im * in_re

    peers, half, _ = arrived_ref.shape
    width = peers * 64
    low = lanes((half, 128)) < 64
    tops, bottoms = [], []
    for m in range(peers // 2):
        a = arrived_ref[2 * m].astype(F32)
        b = arrived_ref[2 * m + 1].astype(F32)
        tops.append(jnp.where(low, a, lane_roll(b, 64)))
        bottoms.append(jnp.where(low, lane_roll(a, 64), b))
    whole = jnp.concatenate(
        [jnp.concatenate(tops, axis=1), jnp.concatenate(bottoms, axis=1)], axis=0
    )
    whole_ref[...] = whole.astype(BF16)
    scale = lax.rsqrt(jnp.sum(whole * whole, axis=1, keepdims=True) / width + 1e-06)
    normed = (whole * scale * gain_ref[...]).astype(BF16)
    drive = dot_nt(normed, w_in_ref[...]).astype(BF16).astype(F32)

    push_re = dot(drive, bbar_re)
    push_im = dot(drive, bbar_im)
    state_re, state_im = state_re_ref[...], state_im_ref[...]
    next_re = abar_re * state_re - abar_im * state_im + push_re
    next_im = abar_re * state_im + abar_im * state_re + push_im
    next_re_ref[...] = next_re
    next_im_ref[...] = next_im
    readout = (
        dot_nt(next_re, blocks(out_re_ref))
        - dot_nt(next_im, blocks(out_im_ref))
        + pass_ref[...] * drive
    )
    mixer = jax.nn.gelu(readout)
    rows = mixer.shape[0] // 4
    packed = jnp.concatenate([mixer[q * rows : (q + 1) * rows] for q in range(4)], axis=1).astype(BF16)
    for t in range(mixer_ref.shape[0]):
        mixer_ref[t] = packed


def targets_row(choice, capacity):
    n = choice.shape[1]
    first, second = choice[0:1, :], choice[1:2, :]
    first_col, second_col = column_of(first), column_of(second)
    earlier = sublanes((n, n)) < lanes((n, n))
    one = jnp.ones((n, n), jnp.int32)
    none = jnp.zeros((n, n), jnp.int32)
    slot_a = jnp.sum(jnp.where((first_col == first) & earlier, one, none), axis=0, keepdims=True)
    slot_b = jnp.sum(
        jnp.where(first_col == second, one, none)
        + jnp.where((second_col == second) & earlier, one, none),
        axis=0,
        keepdims=True,
    )
    return first * capacity + slot_a, second * capacity + slot_b


def dispatch_kernel(
    place_ref, arrived_ref, whole_ref, w_out_ref, gain_ref, choice_ref, sent_ref, own_ref, after_ref
):
    peers, rows, _ = arrived_ref.shape
    width = whole_ref.shape[1]
    lane = lanes((rows, 128))
    quarters = []
    for q in range(4):
        tiles = []
        for m in range(peers // 4):
            tile = None
            for k in range(4):
                piece = lane_roll(arrived_ref[4 * m + k].astype(F32), (k - q) * 32)
                tile = piece if tile is None else jnp.where(lane // 32 == k, piece, tile)
            tiles.append(tile)
        quarters.append(jnp.concatenate(tiles, axis=1))
    mixer = jnp.concatenate(quarters, axis=0).astype(BF16)
    mixed = dot(mixer, w_out_ref[...]).astype(BF16).astype(F32)
    after = (whole_ref[...].astype(F32) + mixed).astype(BF16).astype(F32)
    after_ref[...] = after
    scale = lax.rsqrt(jnp.sum(after * after, axis=1, keepdims=True) / width + 1e-06)
    part = sent_ref.shape[2]
    start = pl.multiple_of(place_ref[0] * part, 128)
    gain = gain_ref[:, pl.ds(start, part)]
    normed = (after_ref[:, pl.ds(start, part)] * scale * gain).astype(BF16)
    experts, capacity, _ = sent_ref.shape
    slots = experts * capacity
    target_a, target_b = targets_row(choice_ref[...], capacity)
    slot = sublanes((slots, whole_ref.shape[0]))
    one = jnp.ones(slot.shape, F32)
    none = jnp.zeros(slot.shape, F32)
    place = jnp.where((slot == target_a) | (slot == target_b), one, none).astype(BF16)
    sent_ref[...] = dot(place, normed).astype(BF16).reshape(experts, capacity, part)
    rank = place_ref[1]
    own = after_ref[:, pl.ds(pl.multiple_of(rank // 2 * 128, 128), 128)]
    odd = jnp.broadcast_to(rank % 2, own.shape) == 1
    own_ref[...] = jnp.where(odd, lane_roll(own, 64), own)


def expert_kernel(piece_ref, gate_ref, up_ref, down_ref, parts_ref):
    count, _, part = piece_ref.shape
    gate = upper = None
    for k in range(count):
        piece = piece_ref[k]
        g = dot(piece, gate_ref[k * part : (k + 1) * part, :])
        u = dot(piece, up_ref[k * part : (k + 1) * part, :])
        gate = g if gate is None else gate + g
        upper = u if upper is None else upper + u
    hidden = (jax.nn.silu(gate) * upper).astype(BF16)
    rows = hidden.shape[0]
    low = lanes((rows, 128)) < 64
    block = 64 * count
    for m in range(part // 128):
        value = dot(hidden, down_ref[:, 2 * m * block : (2 * m + 2) * block])
        for k in range(count):
            a = value[:, k // 2 * 128 : k // 2 * 128 + 128]
            b = value[:, block + k // 2 * 128 : block + k // 2 * 128 + 128]
            if k % 2:
                joined = jnp.where(low, lane_roll(a, 64), b)
            else:
                joined = jnp.where(low, a, lane_roll(b, 64))
            parts_ref[k, :, m * 128 : (m + 1) * 128] = joined.astype(BF16)


def first_sum_kernel(arrived_ref, out_ref):
    total = arrived_ref[0].astype(F32)
    for k in range(1, arrived_ref.shape[0]):
        total = total + arrived_ref[k].astype(F32)
    turned = total.T
    for k in range(out_ref.shape[0]):
        out_ref[k] = turned[k * 64 : (k + 1) * 64, :].astype(BF16)


def slot_of(shape, axis, capacity, half):
    index = lax.broadcasted_iota(jnp.int32, shape, axis)
    short = capacity // 2
    return index // short * capacity + half * short + index % short


def second_sum_kernel(capacity, arrived_ref, out_ref):
    total = arrived_ref[0].astype(F32)
    for k in range(1, arrived_ref.shape[0]):
        total = total + arrived_ref[k].astype(F32)
    total = total.astype(BF16)
    slots = total.shape[1]
    halves = []
    for half in range(2):
        order = slot_of((slots // 2, slots), 0, capacity, half)
        one = jnp.ones(order.shape, F32)
        pick = jnp.where(order == lanes(order.shape), one, jnp.zeros_like(one)).astype(BF16)
        halves.append(dot_nt(pick, total))
    out_ref[...] = jnp.concatenate(halves, axis=1).astype(BF16).reshape(out_ref.shape)


def combine_kernel(capacity, returned_ref, choice_ref, weight_ref, own_ref, out_ref):
    returned = returned_ref[...]
    returned = returned.reshape(returned.shape[0] * returned.shape[1], 128)
    total = own_ref[:, :64]
    weight = weight_ref[...]
    for k, target in enumerate(targets_row(choice_ref[...], capacity)):
        column = column_of(target)
        picked = None
        for half in range(2):
            slot = slot_of((column.shape[0], returned.shape[0]), 1, capacity, half)
            one = jnp.ones(slot.shape, F32)
            pick = jnp.where(slot == column, one, jnp.zeros_like(one)).astype(BF16)
            value = dot(pick, returned)[:, half * 64 : half * 64 + 64]
            picked = value if picked is None else picked + value
        total = total + picked * column_of(weight[k : k + 1, :])
    out_ref[...] = total.astype(BF16)


def body(
    tokens,
    gain_mix,
    w_in,
    decay_rate,
    frequency,
    log_step,
    input_real,
    input_imag,
    readout_real,
    readout_imaginary,
    passthrough_scale,
    state_real,
    state_imag,
    w_out,
    gain_ffn,
    expert_choice,
    expert_weight,
    w_gate,
    w_up,
    w_down,
):
    x_count, y_count, experts = lax.axis_size("x"), lax.axis_size("y"), lax.axis_size("ep")
    tp_count = x_count * y_count
    rows, local_width = tokens.shape
    full_width = local_width * tp_count
    part = full_width // x_count
    capacity = 2 * rows * expert_choice.shape[1] // experts
    slots = experts * capacity
    groups, state = decay_rate.shape
    channels = passthrough_scale.shape[0]
    sds = jax.ShapeDtypeStruct

    copies = call(spread_kernel, sds((tp_count, rows // 2, 128), BF16), tokens)
    arrived = exchange(copies, ("y", "x"))
    whole, next_re, next_im, mixer = call(
        mixer_kernel,
        (
            sds((rows, full_width), BF16),
            sds((rows, groups * state), F32),
            sds((rows, groups * state), F32),
            sds((tp_count, rows // 4, 128), BF16),
        ),
        arrived,
        gain_mix.reshape(1, full_width),
        w_in.T,
        decay_rate,
        frequency,
        log_step,
        jnp.swapaxes(input_real, 1, 2),
        jnp.swapaxes(input_imag, 1, 2),
        readout_real,
        readout_imaginary,
        passthrough_scale.reshape(1, channels),
        state_real.reshape(rows, groups * state),
        state_imag.reshape(rows, groups * state),
        smem=(5,),
    )
    arrived = exchange(mixer, ("y", "x"))
    choice = expert_choice.T
    where = jnp.stack([lax.axis_index("x"), lax.axis_index(("y", "x"))]).astype(jnp.int32)
    sent, own = call(
        dispatch_kernel,
        (sds((experts, capacity, part), BF16), sds((rows, 128), F32)),
        where,
        arrived,
        whole,
        w_out,
        gain_ffn.reshape(1, full_width),
        choice,
        smem=(0,),
        scratch=(pltpu.VMEM((rows, full_width), F32),),
    )
    arrived = exchange(sent, "ep").reshape(slots, part)
    pieces = exchange(jnp.broadcast_to(arrived, (x_count, slots, part)), "x")
    parts = call(
        expert_kernel, sds((x_count, slots, part), BF16), pieces, w_gate[0], w_up[0], w_down[0]
    )
    arrived = exchange(parts, "x")
    halfway = call(first_sum_kernel, sds((y_count, local_width, slots), BF16), arrived)
    arrived = exchange(halfway, "y")
    results = call(
        functools.partial(second_sum_kernel, capacity), sds((experts, capacity // 2, 128), BF16), arrived
    )
    returned = exchange(results, "ep")
    layer_out = call(
        functools.partial(combine_kernel, capacity),
        sds((rows, local_width), BF16),
        returned,
        choice,
        expert_weight.T,
        own,
    )
    shape = state_real.shape
    return (layer_out, next_re.reshape(shape), next_im.reshape(shape))


def solution(mesh):
    tp_count = mesh.shape["tp"]
    devices = mesh.devices.reshape(mesh.shape["ep"], tp_count // X_COUNT, X_COUNT)
    tp = ("y", "x")
    return jax.shard_map(
        body,
        mesh=Mesh(devices, ("ep", "y", "x")),
        in_specs=(
            P("ep", tp),
            P(),
            P(None, tp),
            P(tp, None),
            P(tp, None),
            P(tp),
            P(tp, None, None),
            P(tp, None, None),
            P(tp, None, None),
            P(tp, None, None),
            P(tp),
            P("ep", tp, None),
            P("ep", tp, None),
            P(),
            P(),
            P("ep", None),
            P("ep", None),
            P("ep", None, tp),
            P("ep", None, tp),
            P("ep", tp, None),
        ),
        out_specs=(P("ep", tp), P("ep", tp, None), P("ep", tp, None)),
        check_vma=False,
    )
```

```python
import functools

import jax
import jax.numpy as jnp
from jax import lax
from jax.experimental import pallas as pl
from jax.experimental.pallas import tpu as pltpu
from jax.sharding import Mesh
from jax.sharding import PartitionSpec as P

F32 = jnp.float32
BF16 = jnp.bfloat16
X_COUNT = 4
Y_LOW = 2
TP = ("yh", "yl", "x")
ROWS_OF_TP = ("yh", "yl")
NEAR = ("yl", "x")
FLOPS = 4_000_000_000
VMEM_LIMIT = 16 * 1024 * 1024


def exchange(parts, axis):
    return lax.all_to_all(parts, axis, split_axis=0, concat_axis=0, tiled=True)


def call(kernel, out_shape, *args, smem=(), scratch=(), flops=FLOPS):
    specs = [
        pl.BlockSpec(
            memory_space=pltpu.SMEM if i in smem else pltpu.VMEM
        )
        for i in range(len(args))
    ]
    outs = jax.tree.map(lambda _: pl.BlockSpec(memory_space=pltpu.VMEM), out_shape)
    return pl.pallas_call(
        kernel,
        out_shape=out_shape,
        in_specs=specs,
        out_specs=outs,
        scratch_shapes=list(scratch),
        cost_estimate=pl.CostEstimate(flops=flops, bytes_accessed=0, transcendentals=0),
        compiler_params=pltpu.CompilerParams(vmem_limit_bytes=VMEM_LIMIT),
    )(*args)


def lanes(shape):
    return lax.broadcasted_iota(jnp.int32, shape, len(shape) - 1)


def sublanes(shape):
    return lax.broadcasted_iota(jnp.int32, shape, len(shape) - 2)


def lane_roll(value, amount):
    return pltpu.roll(value, amount % value.shape[-1], value.ndim - 1)


def dot(a, b):
    return jnp.dot(a, b, preferred_element_type=F32)


def dot_nt(a, b):
    return lax.dot_general(a, b, (((1,), (1,)), ((), ())), preferred_element_type=F32)


def column_of(row):
    n = row.shape[-1]
    eye = sublanes((n, n)) == lanes((n, n))
    return jnp.sum(jnp.where(eye, jnp.broadcast_to(row, (n, n)), jnp.zeros((n, n), row.dtype)), axis=1, keepdims=True)


def spread_kernel(tokens_ref, out_ref):
    half = tokens_ref.shape[0] // 2
    values = tokens_ref[...].astype(F32)
    pair = jnp.concatenate([values[:half], values[half:]], axis=1).astype(BF16)
    for t in range(out_ref.shape[0]):
        out_ref[t] = pair


def targets_row(choice, capacity):
    n = choice.shape[1]
    first, second = choice[0:1, :], choice[1:2, :]
    first_col, second_col = column_of(first), column_of(second)
    earlier = sublanes((n, n)) < lanes((n, n))
    one = jnp.ones((n, n), jnp.int32)
    none = jnp.zeros((n, n), jnp.int32)
    slot_a = jnp.sum(jnp.where((first_col == first) & earlier, one, none), axis=0, keepdims=True)
    slot_b = jnp.sum(
        jnp.where(first_col == second, one, none)
        + jnp.where((second_col == second) & earlier, one, none),
        axis=0,
        keepdims=True,
    )
    return first * capacity + slot_a, second * capacity + slot_b


def slot_of(shape, axis, capacity, half):
    index = lax.broadcasted_iota(jnp.int32, shape, axis)
    short = capacity // 2
    return index // short * capacity + half * short + index % short


def prepare_kernel(
    capacity,
    decay_ref,
    freq_ref,
    log_step_ref,
    in_re_ref,
    in_im_ref,
    out_re_ref,
    out_im_ref,
    choice_ref,
    weight_ref,
    factors_ref,
    bbar_ref,
    readout_ref,
    place_ref,
    pick_ref,
    weight_out_ref,
):
    groups, state = decay_ref.shape
    step = jnp.concatenate(
        [jnp.exp(jnp.full((1, state), log_step_ref[g], F32)) for g in range(groups)], axis=1
    )
    decay = jnp.concatenate([decay_ref[g : g + 1, :] for g in range(groups)], axis=1)
    freq = jnp.concatenate([freq_ref[g : g + 1, :] for g in range(groups)], axis=1)
    lam_re = -decay
    magnitude = jnp.exp(lam_re * step)
    abar_re = magnitude * jnp.cos(freq * step)
    abar_im = magnitude * jnp.sin(freq * step)
    denom = lam_re * lam_re + freq * freq
    numer = abar_re - 1.0
    factor_re = (numer * lam_re + abar_im * freq) / denom
    factor_im = (abar_im * lam_re - numer * freq) / denom
    factors_ref[0] = jnp.broadcast_to(abar_re, factors_ref.shape[1:])
    factors_ref[1] = jnp.broadcast_to(abar_im, factors_ref.shape[1:])

    def blocks(ref):
        rows = []
        for g in range(groups):
            zero = jnp.zeros_like(ref[g])
            rows.append(jnp.concatenate([ref[g] if k == g else zero for k in range(groups)], axis=1))
        return jnp.concatenate(rows, axis=0)

    in_re, in_im = blocks(in_re_ref), blocks(in_im_ref)
    bbar_ref[0] = factor_re * in_re - factor_im * in_im
    bbar_ref[1] = factor_re * in_im + factor_im * in_re
    readout_ref[0] = blocks(out_re_ref)
    readout_ref[1] = -blocks(out_im_ref)

    target_a, target_b = targets_row(choice_ref[...], capacity)
    rows = target_a.shape[1]
    slots = place_ref.shape[0]

    def one_hot(condition):
        one = jnp.ones(condition.shape, F32)
        return jnp.where(condition, one, jnp.zeros_like(one)).astype(BF16)

    slot = sublanes((slots, rows))
    place_ref[...] = one_hot((slot == target_a) | (slot == target_b))
    weight = weight_ref[...]
    for k, target in enumerate((target_a, target_b)):
        column = column_of(target)
        for half in range(2):
            order = slot_of((rows, slots // 2), 1, capacity, half)
            pick_ref[2 * k + half] = one_hot(order == column)
        weight_out_ref[k] = jnp.broadcast_to(
            column_of(weight[k : k + 1, :]), weight_out_ref.shape[1:]
        )


def mixer_kernel(
    arrived_ref,
    gain_ref,
    w_in_ref,
    factors_ref,
    bbar_ref,
    readout_ref,
    pass_ref,
    state_re_ref,
    state_im_ref,
    whole_ref,
    next_re_ref,
    next_im_ref,
    mixer_ref,
):
    peers, half, _ = arrived_ref.shape
    width = peers * 64
    low = lanes((half, 128)) < 64
    tops, bottoms = [], []
    for m in range(peers // 2):
        a = arrived_ref[2 * m].astype(F32)
        b = arrived_ref[2 * m + 1].astype(F32)
        tops.append(jnp.where(low, a, lane_roll(b, 64)))
        bottoms.append(jnp.where(low, lane_roll(a, 64), b))
    whole = jnp.concatenate(
        [jnp.concatenate(tops, axis=1), jnp.concatenate(bottoms, axis=1)], axis=0
    )
    whole_ref[...] = whole.astype(BF16)
    scale = lax.rsqrt(jnp.sum(whole * whole, axis=1, keepdims=True) / width + 1e-06)
    normed = (whole * scale * gain_ref[...]).astype(BF16)
    drive = dot_nt(normed, w_in_ref[...]).astype(BF16).astype(F32)

    groups = state_re_ref.shape[1]
    state_re = jnp.concatenate([state_re_ref[:, g, :] for g in range(groups)], axis=1)
    state_im = jnp.concatenate([state_im_ref[:, g, :] for g in range(groups)], axis=1)
    abar_re, abar_im = factors_ref[0, 0:1, :], factors_ref[1, 0:1, :]
    next_re = abar_re * state_re - abar_im * state_im + dot(drive, bbar_ref[0])
    next_im = abar_re * state_im + abar_im * state_re + dot(drive, bbar_ref[1])
    readout = (
        dot_nt(next_re, readout_ref[0]) + dot_nt(next_im, readout_ref[1]) + pass_ref[...] * drive
    )
    mixer = jax.nn.gelu(readout)
    rows = mixer.shape[0] // 4
    packed = jnp.concatenate([mixer[q * rows : (q + 1) * rows] for q in range(4)], axis=1).astype(BF16)
    for t in range(mixer_ref.shape[0]):
        mixer_ref[t] = packed
    state = state_re_ref.shape[2]
    for g in range(groups):
        next_re_ref[:, g, :] = next_re[:, g * state : (g + 1) * state]
        next_im_ref[:, g, :] = next_im[:, g * state : (g + 1) * state]


def dispatch_kernel(
    arrived_ref, whole_ref, w_out_ref, gain_ref, place_ref, sent_ref, own_ref, after_ref
):
    peers, rows, _ = arrived_ref.shape
    width = whole_ref.shape[1]
    lane = lanes((rows, 128))
    quarters = []
    for q in range(4):
        tiles = []
        for m in range(peers // 4):
            tile = None
            for k in range(4):
                piece = lane_roll(arrived_ref[4 * m + k].astype(F32), (k - q) * 32)
                tile = piece if tile is None else jnp.where(lane // 32 == k, piece, tile)
            tiles.append(tile)
        quarters.append(jnp.concatenate(tiles, axis=1))
    mixer = jnp.concatenate(quarters, axis=0).astype(BF16)
    mixed = dot(mixer, w_out_ref[...]).astype(BF16).astype(F32)
    after = (whole_ref[...].astype(F32) + mixed).astype(BF16).astype(F32)
    after_ref[...] = after
    scale = lax.rsqrt(jnp.sum(after * after, axis=1, keepdims=True) / width + 1e-06)
    part = sent_ref.shape[2]
    rank = lax.axis_index(TP)
    start = pl.multiple_of(lax.axis_index(NEAR) * part, 128)
    gain = gain_ref[:, pl.ds(start, part)]
    normed = (after_ref[:, pl.ds(start, part)] * scale * gain).astype(BF16)
    experts, capacity, _ = sent_ref.shape
    sent_ref[...] = dot(place_ref[...], normed).astype(BF16).reshape(experts, capacity, part)
    own = after_ref[:, pl.ds(pl.multiple_of(rank // 2 * 128, 128), 128)]
    odd = jnp.broadcast_to(rank % 2, own.shape) == 1
    own_ref[...] = jnp.where(odd, lane_roll(own, 64), own)


def expert_kernel(piece_ref, gate_ref, up_ref, down_ref, parts_ref):
    pieces, _, share = piece_ref.shape
    count, _, part = parts_ref.shape
    gate = upper = None
    for k in range(pieces):
        piece = piece_ref[k]
        g = dot(piece, gate_ref[k * share : (k + 1) * share, :])
        u = dot(piece, up_ref[k * share : (k + 1) * share, :])
        gate = g if gate is None else gate + g
        upper = u if upper is None else upper + u
    hidden = (jax.nn.silu(gate) * upper).astype(BF16)
    rows = hidden.shape[0]
    low = lanes((rows, 128)) < 64
    block = 64 * count
    for m in range(part // 128):
        value = dot(hidden, down_ref[:, 2 * m * block : (2 * m + 2) * block])
        for k in range(count):
            a = value[:, k // 2 * 128 : k // 2 * 128 + 128]
            b = value[:, block + k // 2 * 128 : block + k // 2 * 128 + 128]
            if k % 2:
                joined = jnp.where(low, lane_roll(a, 64), b)
            else:
                joined = jnp.where(low, a, lane_roll(b, 64))
            parts_ref[k, :, m * 128 : (m + 1) * 128] = joined.astype(BF16)


def first_sum_kernel(arrived_ref, out_ref):
    total = arrived_ref[0].astype(F32)
    for k in range(1, arrived_ref.shape[0]):
        total = total + arrived_ref[k].astype(F32)
    turned = total.T
    for k in range(out_ref.shape[0]):
        out_ref[k] = turned[k * 64 : (k + 1) * 64, :].astype(BF16)


def second_sum_kernel(capacity, arrived_ref, out_ref):
    total = arrived_ref[0].astype(F32)
    for k in range(1, arrived_ref.shape[0]):
        total = total + arrived_ref[k].astype(F32)
    total = total.astype(BF16)
    slots = total.shape[1]
    halves = []
    for half in range(2):
        order = slot_of((slots // 2, slots), 0, capacity, half)
        one = jnp.ones(order.shape, F32)
        pick = jnp.where(order == lanes(order.shape), one, jnp.zeros_like(one)).astype(BF16)
        halves.append(dot_nt(pick, total))
    out_ref[...] = jnp.concatenate(halves, axis=1).astype(BF16).reshape(out_ref.shape)


def combine_kernel(returned_ref, pick_ref, weight_ref, own_ref, out_ref):
    returned = returned_ref[...]
    returned = returned.reshape(returned.shape[0] * returned.shape[1], 128)
    total = own_ref[:, :64]
    for k in range(2):
        picked = dot(pick_ref[2 * k], returned)[:, :64] + dot(pick_ref[2 * k + 1], returned)[:, 64:]
        total = total + picked * weight_ref[k]
    out_ref[...] = total.astype(BF16)


def body(
    tokens,
    gain_mix,
    w_in,
    decay_rate,
    frequency,
    log_step,
    input_real,
    input_imag,
    readout_real,
    readout_imaginary,
    passthrough_scale,
    state_real,
    state_imag,
    w_out,
    gain_ffn,
    expert_choice,
    expert_weight,
    w_gate,
    w_up,
    w_down,
):
    x_count, y_count, experts = lax.axis_size("x"), lax.axis_size(ROWS_OF_TP), lax.axis_size("ep")
    near = lax.axis_size(NEAR)
    tp_count = x_count * y_count
    rows, local_width = tokens.shape
    full_width = local_width * tp_count
    part = full_width // x_count
    share = full_width // near
    capacity = 2 * rows * expert_choice.shape[1] // experts
    slots = experts * capacity
    groups, state = decay_rate.shape
    channels = passthrough_scale.shape[0]
    sds = jax.ShapeDtypeStruct

    copies = call(spread_kernel, sds((tp_count, rows // 2, 128), BF16), tokens)
    arrived = exchange(copies, TP)
    factors, bbar, readout, place, picks, weights = call(
        functools.partial(prepare_kernel, capacity),
        (
            sds((2, 8, groups * state), F32),
            sds((2, channels, groups * state), F32),
            sds((2, channels, groups * state), F32),
            sds((slots, rows), BF16),
            sds((4, rows, slots // 2), BF16),
            sds((2, rows, local_width), F32),
        ),
        decay_rate,
        frequency,
        log_step,
        jnp.swapaxes(input_real, 1, 2),
        jnp.swapaxes(input_imag, 1, 2),
        readout_real,
        readout_imaginary,
        expert_choice.T,
        expert_weight.T,
        smem=(2,),
    )
    whole, next_re, next_im, mixer = call(
        mixer_kernel,
        (
            sds((rows, full_width), BF16),
            sds(state_real.shape, F32),
            sds(state_real.shape, F32),
            sds((tp_count, rows // 4, 128), BF16),
        ),
        arrived,
        gain_mix.reshape(1, full_width),
        w_in.T,
        factors,
        bbar,
        readout,
        passthrough_scale.reshape(1, channels),
        state_real,
        state_imag,
    )
    arrived = exchange(mixer, TP)
    sent, own = call(
        dispatch_kernel,
        (sds((experts, capacity, share), BF16), sds((rows, 128), F32)),
        arrived,
        whole,
        w_out,
        gain_ffn.reshape(1, full_width),
        place,
        scratch=(pltpu.VMEM((rows, full_width), F32),),
    )
    arrived = exchange(sent, "ep").reshape(slots, share)
    pieces = exchange(jnp.broadcast_to(arrived, (near, slots, share)), NEAR)
    parts = call(
        expert_kernel, sds((x_count, slots, part), BF16), pieces, w_gate[0], w_up[0], w_down[0]
    )
    arrived = exchange(parts, "x")
    halfway = call(first_sum_kernel, sds((y_count, local_width, slots), BF16), arrived)
    arrived = exchange(halfway, ROWS_OF_TP)
    results = call(
        functools.partial(second_sum_kernel, capacity), sds((experts, capacity // 2, 128), BF16), arrived
    )
    returned = exchange(results, "ep")
    layer_out = call(
        combine_kernel, sds((rows, local_width), BF16), returned, picks, weights, own
    )
    return (layer_out, next_re, next_im)


def solution(mesh):
    tp_count = mesh.shape["tp"]
    devices = mesh.devices.reshape(
        mesh.shape["ep"], tp_count // (Y_LOW * X_COUNT), Y_LOW, X_COUNT
    )
    tp = TP
    return jax.shard_map(
        body,
        mesh=Mesh(devices, ("ep", *TP)),
        in_specs=(
            P("ep", tp),
            P(),
            P(None, tp),
            P(tp, None),
            P(tp, None),
            P(tp),
            P(tp, None, None),
            P(tp, None, None),
            P(tp, None, None),
            P(tp, None, None),
            P(tp),
            P("ep", tp, None),
            P("ep", tp, None),
            P(),
            P(),
            P("ep", None),
            P("ep", None),
            P("ep", None, tp),
            P("ep", None, tp),
            P("ep", tp, None),
        ),
        out_specs=(P("ep", tp), P("ep", tp, None), P("ep", tp, None)),
        check_vma=False,
    )
```

```python
import functools

import jax
import jax.numpy as jnp
from jax import lax
from jax.experimental import pallas as pl
from jax.experimental.pallas import tpu as pltpu
from jax.sharding import Mesh
from jax.sharding import PartitionSpec as P

F32 = jnp.float32
BF16 = jnp.bfloat16
X_COUNT = 4
Y_LOW = 2
TP = ("yh", "yl", "x")
NEAR = ("yl", "x")
FLOPS = 4_000_000_000
VMEM_LIMIT = 16 * 1024 * 1024


def exchange(parts, axis):
    return lax.all_to_all(parts, axis, split_axis=0, concat_axis=0, tiled=True)


def call(kernel, out_shape, *args, smem=(), scratch=(), flops=FLOPS):
    specs = [
        pl.BlockSpec(
            memory_space=pltpu.SMEM if i in smem else pltpu.VMEM
        )
        for i in range(len(args))
    ]
    outs = jax.tree.map(lambda _: pl.BlockSpec(memory_space=pltpu.VMEM), out_shape)
    return pl.pallas_call(
        kernel,
        out_shape=out_shape,
        in_specs=specs,
        out_specs=outs,
        scratch_shapes=list(scratch),
        cost_estimate=pl.CostEstimate(flops=flops, bytes_accessed=0, transcendentals=0),
        compiler_params=pltpu.CompilerParams(vmem_limit_bytes=VMEM_LIMIT),
    )(*args)


def lanes(shape):
    return lax.broadcasted_iota(jnp.int32, shape, len(shape) - 1)


def sublanes(shape):
    return lax.broadcasted_iota(jnp.int32, shape, len(shape) - 2)


def lane_roll(value, amount):
    return pltpu.roll(value, amount % value.shape[-1], value.ndim - 1)


def dot(a, b):
    return jnp.dot(a, b, preferred_element_type=F32)


def dot_nt(a, b):
    return lax.dot_general(a, b, (((1,), (1,)), ((), ())), preferred_element_type=F32)


def column_of(row):
    n = row.shape[-1]
    eye = sublanes((n, n)) == lanes((n, n))
    return jnp.sum(jnp.where(eye, jnp.broadcast_to(row, (n, n)), jnp.zeros((n, n), row.dtype)), axis=1, keepdims=True)


def spread_kernel(tokens_ref, out_ref):
    half = tokens_ref.shape[0] // 2
    values = tokens_ref[...].astype(F32)
    pair = jnp.concatenate([values[:half], values[half:]], axis=1).astype(BF16)
    for t in range(out_ref.shape[0]):
        out_ref[t] = pair


def targets_row(choice, capacity):
    n = choice.shape[1]
    first, second = choice[0:1, :], choice[1:2, :]
    first_col, second_col = column_of(first), column_of(second)
    earlier = sublanes((n, n)) < lanes((n, n))
    one = jnp.ones((n, n), jnp.int32)
    none = jnp.zeros((n, n), jnp.int32)
    slot_a = jnp.sum(jnp.where((first_col == first) & earlier, one, none), axis=0, keepdims=True)
    slot_b = jnp.sum(
        jnp.where(first_col == second, one, none)
        + jnp.where((second_col == second) & earlier, one, none),
        axis=0,
        keepdims=True,
    )
    return first * capacity + slot_a, second * capacity + slot_b


def slot_of(shape, axis, capacity, half):
    index = lax.broadcasted_iota(jnp.int32, shape, axis)
    short = capacity // 2
    return index // short * capacity + half * short + index % short


def mixer_kernel(
    capacity,
    arrived_ref,
    gain_ref,
    w_in_ref,
    decay_ref,
    freq_ref,
    log_step_ref,
    in_re_ref,
    in_im_ref,
    out_re_ref,
    out_im_ref,
    pass_ref,
    state_re_ref,
    state_im_ref,
    choice_ref,
    weight_ref,
    whole_ref,
    next_re_ref,
    next_im_ref,
    mixer_ref,
    place_ref,
    pick_ref,
    weight_out_ref,
):
    groups, state = decay_ref.shape
    step = jnp.concatenate(
        [jnp.exp(jnp.full((1, state), log_step_ref[g], F32)) for g in range(groups)], axis=1
    )
    decay = jnp.concatenate([decay_ref[g : g + 1, :] for g in range(groups)], axis=1)
    freq = jnp.concatenate([freq_ref[g : g + 1, :] for g in range(groups)], axis=1)
    lam_re = -decay
    magnitude = jnp.exp(lam_re * step)
    abar_re = magnitude * jnp.cos(freq * step)
    abar_im = magnitude * jnp.sin(freq * step)
    denom = lam_re * lam_re + freq * freq
    numer = abar_re - 1.0
    factor_re = (numer * lam_re + abar_im * freq) / denom
    factor_im = (abar_im * lam_re - numer * freq) / denom

    def blocks(ref):
        rows = []
        for g in range(groups):
            zero = jnp.zeros_like(ref[g])
            rows.append(jnp.concatenate([ref[g] if k == g else zero for k in range(groups)], axis=1))
        return jnp.concatenate(rows, axis=0)

    in_re, in_im = blocks(in_re_ref), blocks(in_im_ref)
    bbar_re = factor_re * in_re - factor_im * in_im
    bbar_im = factor_re * in_im + factor_im * in_re

    peers, half, _ = arrived_ref.shape
    width = peers * 64
    low = lanes((half, 128)) < 64
    tops, bottoms = [], []
    for m in range(peers // 2):
        a = arrived_ref[2 * m].astype(F32)
        b = arrived_ref[2 * m + 1].astype(F32)
        tops.append(jnp.where(low, a, lane_roll(b, 64)))
        bottoms.append(jnp.where(low, lane_roll(a, 64), b))
    whole = jnp.concatenate(
        [jnp.concatenate(tops, axis=1), jnp.concatenate(bottoms, axis=1)], axis=0
    )
    whole_ref[...] = whole.astype(BF16)
    scale = lax.rsqrt(jnp.sum(whole * whole, axis=1, keepdims=True) / width + 1e-06)
    normed = (whole * scale * gain_ref[...]).astype(BF16)
    drive = dot_nt(normed, w_in_ref[...]).astype(BF16).astype(F32)

    state_re = jnp.concatenate([state_re_ref[:, g, :] for g in range(groups)], axis=1)
    state_im = jnp.concatenate([state_im_ref[:, g, :] for g in range(groups)], axis=1)
    next_re = abar_re * state_re - abar_im * state_im + dot(drive, bbar_re)
    next_im = abar_re * state_im + abar_im * state_re + dot(drive, bbar_im)
    readout = (
        dot_nt(next_re, blocks(out_re_ref))
        - dot_nt(next_im, blocks(out_im_ref))
        + pass_ref[...] * drive
    )
    mixer = jax.nn.gelu(readout)
    rows = mixer.shape[0] // 4
    packed = jnp.concatenate([mixer[q * rows : (q + 1) * rows] for q in range(4)], axis=1).astype(BF16)
    for t in range(mixer_ref.shape[0]):
        mixer_ref[t] = packed
    state = state_re_ref.shape[2]
    for g in range(groups):
        next_re_ref[:, g, :] = next_re[:, g * state : (g + 1) * state]
        next_im_ref[:, g, :] = next_im[:, g * state : (g + 1) * state]

    target_a, target_b = targets_row(choice_ref[...], capacity)
    tokens = target_a.shape[1]
    slots = place_ref.shape[0]

    def one_hot(condition):
        one = jnp.ones(condition.shape, F32)
        return jnp.where(condition, one, jnp.zeros_like(one)).astype(BF16)

    slot = sublanes((slots, tokens))
    place_ref[...] = one_hot((slot == target_a) | (slot == target_b))
    weight = weight_ref[...]
    for k, target in enumerate((target_a, target_b)):
        column = column_of(target)
        for half in range(2):
            order = slot_of((tokens, slots // 2), 1, capacity, half)
            pick_ref[2 * k + half] = one_hot(order == column)
        weight_out_ref[k] = jnp.broadcast_to(
            column_of(weight[k : k + 1, :]), weight_out_ref.shape[1:]
        )


def dispatch_kernel(
    arrived_ref, whole_ref, w_out_ref, gain_ref, place_ref, sent_ref, own_ref, after_ref
):
    peers, rows, _ = arrived_ref.shape
    width = whole_ref.shape[1]
    lane = lanes((rows, 128))
    quarters = []
    for q in range(4):
        tiles = []
        for m in range(peers // 4):
            tile = None
            for k in range(4):
                piece = lane_roll(arrived_ref[4 * m + k].astype(F32), (k - q) * 32)
                tile = piece if tile is None else jnp.where(lane // 32 == k, piece, tile)
            tiles.append(tile)
        quarters.append(jnp.concatenate(tiles, axis=1))
    mixer = jnp.concatenate(quarters, axis=0).astype(BF16)
    mixed = dot(mixer, w_out_ref[...]).astype(BF16).astype(F32)
    after = (whole_ref[...].astype(F32) + mixed).astype(BF16).astype(F32)
    after_ref[...] = after
    scale = lax.rsqrt(jnp.sum(after * after, axis=1, keepdims=True) / width + 1e-06)
    part = sent_ref.shape[2]
    rank = lax.axis_index(TP)
    start = pl.multiple_of(lax.axis_index(NEAR) * part, 128)
    gain = gain_ref[:, pl.ds(start, part)]
    normed = (after_ref[:, pl.ds(start, part)] * scale * gain).astype(BF16)
    experts, capacity, _ = sent_ref.shape
    sent_ref[...] = dot(place_ref[...], normed).astype(BF16).reshape(experts, capacity, part)
    own = after_ref[:, pl.ds(pl.multiple_of(rank // 2 * 128, 128), 128)]
    odd = jnp.broadcast_to(rank % 2, own.shape) == 1
    own_ref[...] = jnp.where(odd, lane_roll(own, 64), own)


def expert_kernel(piece_ref, gate_ref, up_ref, down_ref, parts_ref):
    pieces, _, share = piece_ref.shape
    count, _, part = parts_ref.shape
    gate = upper = None
    for k in range(pieces):
        piece = piece_ref[k]
        g = dot(piece, gate_ref[k * share : (k + 1) * share, :])
        u = dot(piece, up_ref[k * share : (k + 1) * share, :])
        gate = g if gate is None else gate + g
        upper = u if upper is None else upper + u
    hidden = (jax.nn.silu(gate) * upper).astype(BF16)
    rows = hidden.shape[0]
    low = lanes((rows, 128)) < 64
    block = 64 * count
    for m in range(part // 128):
        value = dot(hidden, down_ref[:, 2 * m * block : (2 * m + 2) * block])
        for k in range(count):
            a = value[:, k // 2 * 128 : k // 2 * 128 + 128]
            b = value[:, block + k // 2 * 128 : block + k // 2 * 128 + 128]
            if k % 2:
                joined = jnp.where(low, lane_roll(a, 64), b)
            else:
                joined = jnp.where(low, a, lane_roll(b, 64))
            parts_ref[k, :, m * 128 : (m + 1) * 128] = joined.astype(BF16)


def sum_kernel(capacity, arrived_ref, out_ref):
    total = arrived_ref[0].astype(F32)
    for k in range(1, arrived_ref.shape[0]):
        total = total + arrived_ref[k].astype(F32)
    total = total.astype(BF16)
    slots = total.shape[0]
    halves = []
    for half in range(2):
        order = slot_of((slots // 2, slots), 0, capacity, half)
        one = jnp.ones(order.shape, F32)
        pick = jnp.where(order == lanes(order.shape), one, jnp.zeros_like(one)).astype(BF16)
        halves.append(dot(pick, total))
    first, second = halves
    experts, rows, short, _ = out_ref.shape
    low = lanes((slots // 2, 128)) < 64
    for m in range(rows // 2):
        a = first[:, m * 128 : (m + 1) * 128]
        b = second[:, m * 128 : (m + 1) * 128]
        even = jnp.where(low, a, lane_roll(b, 64)).astype(BF16)
        odd = jnp.where(low, lane_roll(a, 64), b).astype(BF16)
        out_ref[:, 2 * m] = even.reshape(experts, short, 128)
        out_ref[:, 2 * m + 1] = odd.reshape(experts, short, 128)


def combine_kernel(returned_ref, pick_ref, weight_ref, own_ref, out_ref):
    experts, rows, short, _ = returned_ref.shape
    returned = returned_ref[:, 0].astype(F32)
    for k in range(1, rows):
        returned = returned + returned_ref[:, k].astype(F32)
    returned = returned.reshape(experts * short, 128).astype(BF16)
    total = own_ref[:, :64]
    for k in range(2):
        picked = dot(pick_ref[2 * k], returned)[:, :64] + dot(pick_ref[2 * k + 1], returned)[:, 64:]
        total = total + picked * weight_ref[k]
    out_ref[...] = total.astype(BF16)


def body(
    tokens,
    gain_mix,
    w_in,
    decay_rate,
    frequency,
    log_step,
    input_real,
    input_imag,
    readout_real,
    readout_imaginary,
    passthrough_scale,
    state_real,
    state_imag,
    w_out,
    gain_ffn,
    expert_choice,
    expert_weight,
    w_gate,
    w_up,
    w_down,
):
    near, far, experts = lax.axis_size(NEAR), lax.axis_size("yh"), lax.axis_size("ep")
    tp_count = near * far
    rows, local_width = tokens.shape
    full_width = local_width * tp_count
    share = full_width // near
    capacity = 2 * rows * expert_choice.shape[1] // experts
    slots = experts * capacity
    groups, state = decay_rate.shape
    channels = passthrough_scale.shape[0]
    sds = jax.ShapeDtypeStruct

    copies = call(spread_kernel, sds((tp_count, rows // 2, 128), BF16), tokens)
    arrived = exchange(copies, TP)
    whole, next_re, next_im, mixer, place, picks, weights = call(
        functools.partial(mixer_kernel, capacity),
        (
            sds((rows, full_width), BF16),
            sds(state_real.shape, F32),
            sds(state_real.shape, F32),
            sds((tp_count, rows // 4, 128), BF16),
            sds((slots, rows), BF16),
            sds((4, rows, slots // 2), BF16),
            sds((2, rows, local_width), F32),
        ),
        arrived,
        gain_mix.reshape(1, full_width),
        w_in.T,
        decay_rate,
        frequency,
        log_step,
        jnp.swapaxes(input_real, 1, 2),
        jnp.swapaxes(input_imag, 1, 2),
        readout_real,
        readout_imaginary,
        passthrough_scale.reshape(1, channels),
        state_real,
        state_imag,
        expert_choice.T,
        expert_weight.T,
        smem=(5,),
    )
    arrived = exchange(mixer, TP)
    sent, own = call(
        dispatch_kernel,
        (sds((experts, capacity, share), BF16), sds((rows, 128), F32)),
        arrived,
        whole,
        w_out,
        gain_ffn.reshape(1, full_width),
        place,
        scratch=(pltpu.VMEM((rows, full_width), F32),),
    )
    arrived = exchange(sent, "ep").reshape(slots, share)
    pieces = exchange(jnp.broadcast_to(arrived, (near, slots, share)), NEAR)
    parts = call(
        expert_kernel,
        sds((near, slots, far * local_width), BF16),
        pieces,
        w_gate[0],
        w_up[0],
        w_down[0],
    )
    arrived = exchange(parts, NEAR)
    short = capacity // 2
    results = call(
        functools.partial(sum_kernel, capacity), sds((experts, far, short, 128), BF16), arrived
    )
    returned = exchange(results.reshape(experts * far, short, 128), ("ep", "yh"))
    returned = returned.reshape(experts, far, short, 128)
    layer_out = call(
        combine_kernel, sds((rows, local_width), BF16), returned, picks, weights, own
    )
    return (layer_out, next_re, next_im)


def solution(mesh):
    tp_count = mesh.shape["tp"]
    devices = mesh.devices.reshape(
        mesh.shape["ep"], tp_count // (Y_LOW * X_COUNT), Y_LOW, X_COUNT
    )
    tp = TP
    return jax.shard_map(
        body,
        mesh=Mesh(devices, ("ep", *TP)),
        in_specs=(
            P("ep", tp),
            P(),
            P(None, tp),
            P(tp, None),
            P(tp, None),
            P(tp),
            P(tp, None, None),
            P(tp, None, None),
            P(tp, None, None),
            P(tp, None, None),
            P(tp),
            P("ep", tp, None),
            P("ep", tp, None),
            P(),
            P(),
            P("ep", None),
            P("ep", None),
            P("ep", None, tp),
            P("ep", None, tp),
            P("ep", tp, None),
        ),
        out_specs=(P("ep", tp), P("ep", tp, None), P("ep", tp, None)),
        check_vma=False,
    )
```

```python
import functools

import jax
import jax.numpy as jnp
from jax import lax
from jax.experimental import pallas as pl
from jax.experimental.pallas import tpu as pltpu
from jax.sharding import Mesh
from jax.sharding import PartitionSpec as P

F32 = jnp.float32
BF16 = jnp.bfloat16
X_COUNT = 4
Y_LOW = 2
TP = ("yh", "yl", "x")
NEAR = ("yl", "x")
FLOPS = 4_000_000_000
VMEM_LIMIT = 16 * 1024 * 1024


def exchange(parts, axis):
    return lax.all_to_all(parts, axis, split_axis=0, concat_axis=0, tiled=True)


def call(kernel, out_shape, *args, smem=(), hbm_outs=(), scratch=(), flops=FLOPS):
    specs = [
        pl.BlockSpec(
            memory_space=pltpu.SMEM if i in smem else pltpu.VMEM
        )
        for i in range(len(args))
    ]
    if isinstance(out_shape, tuple):
        outs = tuple(
            pl.BlockSpec(memory_space=pltpu.HBM if i in hbm_outs else pltpu.VMEM)
            for i in range(len(out_shape))
        )
    else:
        outs = pl.BlockSpec(memory_space=pltpu.VMEM)
    return pl.pallas_call(
        kernel,
        out_shape=out_shape,
        in_specs=specs,
        out_specs=outs,
        scratch_shapes=list(scratch),
        cost_estimate=pl.CostEstimate(flops=flops, bytes_accessed=0, transcendentals=0),
        compiler_params=pltpu.CompilerParams(vmem_limit_bytes=VMEM_LIMIT),
    )(*args)


def lanes(shape):
    return lax.broadcasted_iota(jnp.int32, shape, len(shape) - 1)


def sublanes(shape):
    return lax.broadcasted_iota(jnp.int32, shape, len(shape) - 2)


def lane_roll(value, amount):
    return pltpu.roll(value, amount % value.shape[-1], value.ndim - 1)


def dot(a, b):
    return jnp.dot(a, b, preferred_element_type=F32)


def dot_nt(a, b):
    return lax.dot_general(a, b, (((1,), (1,)), ((), ())), preferred_element_type=F32)


def column_of(row):
    n = row.shape[-1]
    eye = sublanes((n, n)) == lanes((n, n))
    return jnp.sum(jnp.where(eye, jnp.broadcast_to(row, (n, n)), jnp.zeros((n, n), row.dtype)), axis=1, keepdims=True)


def spread_kernel(tokens_ref, out_ref):
    half = tokens_ref.shape[0] // 2
    values = tokens_ref[...].astype(F32)
    pair = jnp.concatenate([values[:half], values[half:]], axis=1).astype(BF16)
    for t in range(out_ref.shape[0]):
        out_ref[t] = pair


def targets_row(choice, capacity):
    n = choice.shape[1]
    first, second = choice[0:1, :], choice[1:2, :]
    first_col, second_col = column_of(first), column_of(second)
    earlier = sublanes((n, n)) < lanes((n, n))
    one = jnp.ones((n, n), jnp.int32)
    none = jnp.zeros((n, n), jnp.int32)
    slot_a = jnp.sum(jnp.where((first_col == first) & earlier, one, none), axis=0, keepdims=True)
    slot_b = jnp.sum(
        jnp.where(first_col == second, one, none)
        + jnp.where((second_col == second) & earlier, one, none),
        axis=0,
        keepdims=True,
    )
    return first * capacity + slot_a, second * capacity + slot_b


def slot_of(shape, axis, capacity, half):
    index = lax.broadcasted_iota(jnp.int32, shape, axis)
    short = capacity // 2
    return index // short * capacity + half * short + index % short


def mixer_kernel(
    arrived_ref,
    gain_ref,
    w_in_ref,
    decay_ref,
    freq_ref,
    log_step_ref,
    in_re_ref,
    in_im_ref,
    out_re_ref,
    out_im_ref,
    pass_ref,
    state_re_ref,
    state_im_ref,
    whole_ref,
    next_re_ref,
    next_im_ref,
    mixer_ref,
):
    groups, state = decay_ref.shape
    step = jnp.concatenate(
        [jnp.exp(jnp.full((1, state), log_step_ref[g], F32)) for g in range(groups)], axis=1
    )
    decay = jnp.concatenate([decay_ref[g : g + 1, :] for g in range(groups)], axis=1)
    freq = jnp.concatenate([freq_ref[g : g + 1, :] for g in range(groups)], axis=1)
    lam_re = -decay
    magnitude = jnp.exp(lam_re * step)
    abar_re = magnitude * jnp.cos(freq * step)
    abar_im = magnitude * jnp.sin(freq * step)
    denom = lam_re * lam_re + freq * freq
    numer = abar_re - 1.0
    factor_re = (numer * lam_re + abar_im * freq) / denom
    factor_im = (abar_im * lam_re - numer * freq) / denom

    def blocks(ref):
        rows = []
        for g in range(groups):
            zero = jnp.zeros_like(ref[g])
            rows.append(jnp.concatenate([ref[g] if k == g else zero for k in range(groups)], axis=1))
        return jnp.concatenate(rows, axis=0)

    in_re, in_im = blocks(in_re_ref), blocks(in_im_ref)
    bbar_re = factor_re * in_re - factor_im * in_im
    bbar_im = factor_re * in_im + factor_im * in_re

    peers, half, _ = arrived_ref.shape
    width = peers * 64
    low = lanes((half, 128)) < 64
    tops, bottoms = [], []
    for m in range(peers // 2):
        a = arrived_ref[2 * m].astype(F32)
        b = arrived_ref[2 * m + 1].astype(F32)
        tops.append(jnp.where(low, a, lane_roll(b, 64)))
        bottoms.append(jnp.where(low, lane_roll(a, 64), b))
    whole = jnp.concatenate(
        [jnp.concatenate(tops, axis=1), jnp.concatenate(bottoms, axis=1)], axis=0
    )
    whole_ref[...] = whole.astype(BF16)
    scale = lax.rsqrt(jnp.sum(whole * whole, axis=1, keepdims=True) / width + 1e-06)
    normed = (whole * scale * gain_ref[...]).astype(BF16)
    drive = dot_nt(normed, w_in_ref[...]).astype(BF16).astype(F32)

    state_re = jnp.concatenate([state_re_ref[:, g, :] for g in range(groups)], axis=1)
    state_im = jnp.concatenate([state_im_ref[:, g, :] for g in range(groups)], axis=1)
    next_re = abar_re * state_re - abar_im * state_im + dot(drive, bbar_re)
    next_im = abar_re * state_im + abar_im * state_re + dot(drive, bbar_im)
    readout = (
        dot_nt(next_re, blocks(out_re_ref))
        - dot_nt(next_im, blocks(out_im_ref))
        + pass_ref[...] * drive
    )
    mixer = jax.nn.gelu(readout)
    rows = mixer.shape[0] // 4
    packed = jnp.concatenate([mixer[q * rows : (q + 1) * rows] for q in range(4)], axis=1).astype(BF16)
    for t in range(mixer_ref.shape[0]):
        mixer_ref[t] = packed
    state = state_re_ref.shape[2]
    for g in range(groups):
        next_re_ref[:, g, :] = next_re[:, g * state : (g + 1) * state]
        next_im_ref[:, g, :] = next_im[:, g * state : (g + 1) * state]


def dispatch_kernel(
    arrived_ref,
    whole_ref,
    w_out_ref,
    gain_ref,
    choice_ref,
    weight_ref,
    state_re_ref,
    state_im_ref,
    sent_ref,
    own_ref,
    pick_ref,
    weight_out_ref,
    out_re_ref,
    out_im_ref,
    after_ref,
    sems,
):
    copies = [
        pltpu.make_async_copy(state_re_ref, out_re_ref, sems.at[0]),
        pltpu.make_async_copy(state_im_ref, out_im_ref, sems.at[1]),
    ]
    for copy in copies:
        copy.start()
    experts, capacity, _ = sent_ref.shape
    target_a, target_b = targets_row(choice_ref[...], capacity)
    tokens = target_a.shape[1]
    slots = experts * capacity

    def one_hot(condition):
        one = jnp.ones(condition.shape, F32)
        return jnp.where(condition, one, jnp.zeros_like(one)).astype(BF16)

    slot = sublanes((slots, tokens))
    place = one_hot((slot == target_a) | (slot == target_b))
    weight = weight_ref[...]
    for k, target in enumerate((target_a, target_b)):
        column = column_of(target)
        for half in range(2):
            order = slot_of((tokens, slots // 2), 1, capacity, half)
            pick_ref[2 * k + half] = one_hot(order == column)
        weight_out_ref[k] = jnp.broadcast_to(
            column_of(weight[k : k + 1, :]), weight_out_ref.shape[1:]
        )
    peers, rows, _ = arrived_ref.shape
    width = whole_ref.shape[1]
    lane = lanes((rows, 128))
    quarters = []
    for q in range(4):
        tiles = []
        for m in range(peers // 4):
            tile = None
            for k in range(4):
                piece = lane_roll(arrived_ref[4 * m + k].astype(F32), (k - q) * 32)
                tile = piece if tile is None else jnp.where(lane // 32 == k, piece, tile)
            tiles.append(tile)
        quarters.append(jnp.concatenate(tiles, axis=1))
    mixer = jnp.concatenate(quarters, axis=0).astype(BF16)
    mixed = dot(mixer, w_out_ref[...]).astype(BF16).astype(F32)
    after = (whole_ref[...].astype(F32) + mixed).astype(BF16).astype(F32)
    after_ref[...] = after
    scale = lax.rsqrt(jnp.sum(after * after, axis=1, keepdims=True) / width + 1e-06)
    part = sent_ref.shape[2]
    rank = lax.axis_index(TP)
    start = pl.multiple_of(lax.axis_index(NEAR) * part, 128)
    gain = gain_ref[:, pl.ds(start, part)]
    normed = (after_ref[:, pl.ds(start, part)] * scale * gain).astype(BF16)
    sent_ref[...] = dot(place, normed).astype(BF16).reshape(experts, capacity, part)
    own = after_ref[:, pl.ds(pl.multiple_of(rank // 2 * 128, 128), 128)]
    odd = jnp.broadcast_to(rank % 2, own.shape) == 1
    own_ref[...] = jnp.where(odd, lane_roll(own, 64), own)
    for copy in copies:
        copy.wait()


def expert_kernel(piece_ref, gate_ref, up_ref, down_ref, parts_ref):
    pieces, _, share = piece_ref.shape
    count, _, part = parts_ref.shape
    gate = upper = None
    for k in range(pieces):
        piece = piece_ref[k]
        g = dot(piece, gate_ref[k * share : (k + 1) * share, :])
        u = dot(piece, up_ref[k * share : (k + 1) * share, :])
        gate = g if gate is None else gate + g
        upper = u if upper is None else upper + u
    hidden = (jax.nn.silu(gate) * upper).astype(BF16)
    rows = hidden.shape[0]
    low = lanes((rows, 128)) < 64
    block = 64 * count
    for m in range(part // 128):
        value = dot(hidden, down_ref[:, 2 * m * block : (2 * m + 2) * block])
        for k in range(count):
            a = value[:, k // 2 * 128 : k // 2 * 128 + 128]
            b = value[:, block + k // 2 * 128 : block + k // 2 * 128 + 128]
            if k % 2:
                joined = jnp.where(low, lane_roll(a, 64), b)
            else:
                joined = jnp.where(low, a, lane_roll(b, 64))
            parts_ref[k, :, m * 128 : (m + 1) * 128] = joined.astype(BF16)


def sum_kernel(capacity, arrived_ref, out_ref):
    total = arrived_ref[0].astype(F32)
    for k in range(1, arrived_ref.shape[0]):
        total = total + arrived_ref[k].astype(F32)
    total = total.astype(BF16)
    slots = total.shape[0]
    halves = []
    for half in range(2):
        order = slot_of((slots // 2, slots), 0, capacity, half)
        one = jnp.ones(order.shape, F32)
        pick = jnp.where(order == lanes(order.shape), one, jnp.zeros_like(one)).astype(BF16)
        halves.append(dot(pick, total))
    first, second = halves
    experts, rows, short, _ = out_ref.shape
    low = lanes((slots // 2, 128)) < 64
    for m in range(rows // 2):
        a = first[:, m * 128 : (m + 1) * 128]
        b = second[:, m * 128 : (m + 1) * 128]
        even = jnp.where(low, a, lane_roll(b, 64)).astype(BF16)
        odd = jnp.where(low, lane_roll(a, 64), b).astype(BF16)
        out_ref[:, 2 * m] = even.reshape(experts, short, 128)
        out_ref[:, 2 * m + 1] = odd.reshape(experts, short, 128)


def combine_kernel(returned_ref, pick_ref, weight_ref, own_ref, out_ref):
    experts, rows, short, _ = returned_ref.shape
    returned = returned_ref[:, 0].astype(F32)
    for k in range(1, rows):
        returned = returned + returned_ref[:, k].astype(F32)
    returned = returned.reshape(experts * short, 128).astype(BF16)
    total = own_ref[:, :64]
    for k in range(2):
        picked = dot(pick_ref[2 * k], returned)[:, :64] + dot(pick_ref[2 * k + 1], returned)[:, 64:]
        total = total + picked * weight_ref[k]
    out_ref[...] = total.astype(BF16)


def body(
    tokens,
    gain_mix,
    w_in,
    decay_rate,
    frequency,
    log_step,
    input_real,
    input_imag,
    readout_real,
    readout_imaginary,
    passthrough_scale,
    state_real,
    state_imag,
    w_out,
    gain_ffn,
    expert_choice,
    expert_weight,
    w_gate,
    w_up,
    w_down,
):
    near, far, experts = lax.axis_size(NEAR), lax.axis_size("yh"), lax.axis_size("ep")
    tp_count = near * far
    rows, local_width = tokens.shape
    full_width = local_width * tp_count
    share = full_width // near
    capacity = 2 * rows * expert_choice.shape[1] // experts
    slots = experts * capacity
    groups, state = decay_rate.shape
    channels = passthrough_scale.shape[0]
    sds = jax.ShapeDtypeStruct

    copies = call(spread_kernel, sds((tp_count, rows // 2, 128), BF16), tokens)
    arrived = exchange(copies, TP)
    whole, next_re, next_im, mixer = call(
        mixer_kernel,
        (
            sds((rows, full_width), BF16),
            sds(state_real.shape, F32),
            sds(state_real.shape, F32),
            sds((tp_count, rows // 4, 128), BF16),
        ),
        arrived,
        gain_mix.reshape(1, full_width),
        w_in.T,
        decay_rate,
        frequency,
        log_step,
        jnp.swapaxes(input_real, 1, 2),
        jnp.swapaxes(input_imag, 1, 2),
        readout_real,
        readout_imaginary,
        passthrough_scale.reshape(1, channels),
        state_real,
        state_imag,
        smem=(5,),
    )
    arrived = exchange(mixer, TP)
    sent, own, picks, weights, next_re, next_im = call(
        dispatch_kernel,
        (
            sds((experts, capacity, share), BF16),
            sds((rows, 128), F32),
            sds((4, rows, slots // 2), BF16),
            sds((2, rows, local_width), F32),
            sds(state_real.shape, F32),
            sds(state_real.shape, F32),
        ),
        arrived,
        whole,
        w_out,
        gain_ffn.reshape(1, full_width),
        expert_choice.T,
        expert_weight.T,
        next_re,
        next_im,
        hbm_outs=(4, 5),
        scratch=(pltpu.VMEM((rows, full_width), F32), pltpu.SemaphoreType.DMA((2,))),
    )
    arrived = exchange(sent, "ep").reshape(slots, share)
    pieces = exchange(jnp.broadcast_to(arrived, (near, slots, share)), NEAR)
    parts = call(
        expert_kernel,
        sds((near, slots, far * local_width), BF16),
        pieces,
        w_gate[0],
        w_up[0],
        w_down[0],
    )
    arrived = exchange(parts, NEAR)
    short = capacity // 2
    results = call(
        functools.partial(sum_kernel, capacity), sds((experts, far, short, 128), BF16), arrived
    )
    returned = exchange(results.reshape(experts * far, short, 128), ("ep", "yh"))
    returned = returned.reshape(experts, far, short, 128)
    layer_out = call(
        combine_kernel, sds((rows, local_width), BF16), returned, picks, weights, own
    )
    return (layer_out, next_re, next_im)


def solution(mesh):
    tp_count = mesh.shape["tp"]
    devices = mesh.devices.reshape(
        mesh.shape["ep"], tp_count // (Y_LOW * X_COUNT), Y_LOW, X_COUNT
    )
    tp = TP
    return jax.shard_map(
        body,
        mesh=Mesh(devices, ("ep", *TP)),
        in_specs=(
            P("ep", tp),
            P(),
            P(None, tp),
            P(tp, None),
            P(tp, None),
            P(tp),
            P(tp, None, None),
            P(tp, None, None),
            P(tp, None, None),
            P(tp, None, None),
            P(tp),
            P("ep", tp, None),
            P("ep", tp, None),
            P(),
            P(),
            P("ep", None),
            P("ep", None),
            P("ep", None, tp),
            P("ep", None, tp),
            P("ep", tp, None),
        ),
        out_specs=(P("ep", tp), P("ep", tp, None), P("ep", tp, None)),
        check_vma=False,
    )
```

```python
import functools

import jax
import jax.numpy as jnp
from jax import lax
from jax.experimental import pallas as pl
from jax.experimental.pallas import tpu as pltpu
from jax.sharding import Mesh
from jax.sharding import PartitionSpec as P

F32 = jnp.float32
BF16 = jnp.bfloat16
X_COUNT = 4
Y_LOW = 2
TP = ("yh", "yl", "x")
NEAR = ("yl", "x")
FLOPS = 4_000_000_000
VMEM_LIMIT = 16 * 1024 * 1024


def exchange(parts, axis):
    return lax.all_to_all(parts, axis, split_axis=0, concat_axis=0, tiled=True)


def call(kernel, out_shape, *args, smem=(), hbm_outs=(), scratch=(), flops=FLOPS):
    specs = [
        pl.BlockSpec(
            memory_space=pltpu.SMEM if i in smem else pltpu.VMEM
        )
        for i in range(len(args))
    ]
    if isinstance(out_shape, tuple):
        outs = tuple(
            pl.BlockSpec(memory_space=pltpu.HBM if i in hbm_outs else pltpu.VMEM)
            for i in range(len(out_shape))
        )
    else:
        outs = pl.BlockSpec(memory_space=pltpu.VMEM)
    return pl.pallas_call(
        kernel,
        out_shape=out_shape,
        in_specs=specs,
        out_specs=outs,
        scratch_shapes=list(scratch),
        cost_estimate=pl.CostEstimate(flops=flops, bytes_accessed=0, transcendentals=0),
        compiler_params=pltpu.CompilerParams(vmem_limit_bytes=VMEM_LIMIT),
    )(*args)


def lanes(shape):
    return lax.broadcasted_iota(jnp.int32, shape, len(shape) - 1)


def sublanes(shape):
    return lax.broadcasted_iota(jnp.int32, shape, len(shape) - 2)


def lane_roll(value, amount):
    return pltpu.roll(value, amount % value.shape[-1], value.ndim - 1)


def dot(a, b):
    return jnp.dot(a, b, preferred_element_type=F32)


def dot_nt(a, b):
    return lax.dot_general(a, b, (((1,), (1,)), ((), ())), preferred_element_type=F32)


def column_of(row):
    n = row.shape[-1]
    eye = sublanes((n, n)) == lanes((n, n))
    return jnp.sum(jnp.where(eye, jnp.broadcast_to(row, (n, n)), jnp.zeros((n, n), row.dtype)), axis=1, keepdims=True)


def spread_kernel(tokens_ref, out_ref):
    half = tokens_ref.shape[0] // 2
    values = tokens_ref[...].astype(F32)
    pair = jnp.concatenate([values[:half], values[half:]], axis=1).astype(BF16)
    for t in range(out_ref.shape[0]):
        out_ref[t] = pair


def targets_row(choice, capacity):
    n = choice.shape[1]
    first, second = choice[0:1, :], choice[1:2, :]
    first_col, second_col = column_of(first), column_of(second)
    earlier = sublanes((n, n)) < lanes((n, n))
    one = jnp.ones((n, n), jnp.int32)
    none = jnp.zeros((n, n), jnp.int32)
    slot_a = jnp.sum(jnp.where((first_col == first) & earlier, one, none), axis=0, keepdims=True)
    slot_b = jnp.sum(
        jnp.where(first_col == second, one, none)
        + jnp.where((second_col == second) & earlier, one, none),
        axis=0,
        keepdims=True,
    )
    return first * capacity + slot_a, second * capacity + slot_b


def slot_of(shape, axis, capacity, half):
    index = lax.broadcasted_iota(jnp.int32, shape, axis)
    short = capacity // 2
    return index // short * capacity + half * short + index % short


def mixer_kernel(
    arrived_ref,
    gain_ref,
    w_in_ref,
    decay_ref,
    freq_ref,
    log_step_ref,
    in_re_ref,
    in_im_ref,
    out_re_ref,
    out_im_ref,
    pass_ref,
    state_re_ref,
    state_im_ref,
    whole_ref,
    next_re_ref,
    next_im_ref,
    mixer_ref,
):
    groups, state = decay_ref.shape
    step = jnp.concatenate(
        [jnp.exp(jnp.full((1, state), log_step_ref[g], F32)) for g in range(groups)], axis=1
    )
    decay = jnp.concatenate([decay_ref[g : g + 1, :] for g in range(groups)], axis=1)
    freq = jnp.concatenate([freq_ref[g : g + 1, :] for g in range(groups)], axis=1)
    lam_re = -decay
    magnitude = jnp.exp(lam_re * step)
    abar_re = magnitude * jnp.cos(freq * step)
    abar_im = magnitude * jnp.sin(freq * step)
    denom = lam_re * lam_re + freq * freq
    numer = abar_re - 1.0
    factor_re = (numer * lam_re + abar_im * freq) / denom
    factor_im = (abar_im * lam_re - numer * freq) / denom

    def blocks(ref):
        rows = []
        for g in range(groups):
            zero = jnp.zeros_like(ref[g])
            rows.append(jnp.concatenate([ref[g] if k == g else zero for k in range(groups)], axis=1))
        return jnp.concatenate(rows, axis=0)

    in_re, in_im = blocks(in_re_ref), blocks(in_im_ref)
    bbar_re = factor_re * in_re - factor_im * in_im
    bbar_im = factor_re * in_im + factor_im * in_re

    peers, half, _ = arrived_ref.shape
    width = peers * 64
    low = lanes((half, 128)) < 64
    tops, bottoms = [], []
    for m in range(peers // 2):
        a = arrived_ref[2 * m].astype(F32)
        b = arrived_ref[2 * m + 1].astype(F32)
        tops.append(jnp.where(low, a, lane_roll(b, 64)))
        bottoms.append(jnp.where(low, lane_roll(a, 64), b))
    whole = jnp.concatenate(
        [jnp.concatenate(tops, axis=1), jnp.concatenate(bottoms, axis=1)], axis=0
    )
    whole_ref[...] = whole.astype(BF16)
    scale = lax.rsqrt(jnp.sum(whole * whole, axis=1, keepdims=True) / width + 1e-06)
    normed = (whole * scale * gain_ref[...]).astype(BF16)
    drive = dot_nt(normed, w_in_ref[...]).astype(BF16).astype(F32)

    state_re = jnp.concatenate([state_re_ref[:, g, :] for g in range(groups)], axis=1)
    state_im = jnp.concatenate([state_im_ref[:, g, :] for g in range(groups)], axis=1)
    next_re = abar_re * state_re - abar_im * state_im + dot(drive, bbar_re)
    next_im = abar_re * state_im + abar_im * state_re + dot(drive, bbar_im)
    readout = (
        dot_nt(next_re, blocks(out_re_ref))
        - dot_nt(next_im, blocks(out_im_ref))
        + pass_ref[...] * drive
    )
    mixer = jax.nn.gelu(readout)
    rows = mixer.shape[0] // 4
    packed = jnp.concatenate([mixer[q * rows : (q + 1) * rows] for q in range(4)], axis=1).astype(BF16)
    for t in range(mixer_ref.shape[0]):
        mixer_ref[t] = packed
    state = state_re_ref.shape[2]
    for g in range(groups):
        next_re_ref[:, g, :] = next_re[:, g * state : (g + 1) * state]
        next_im_ref[:, g, :] = next_im[:, g * state : (g + 1) * state]


def dispatch_kernel(
    arrived_ref,
    whole_ref,
    w_out_ref,
    gain_ref,
    choice_ref,
    weight_ref,
    sent_ref,
    own_ref,
    pick_ref,
    weight_out_ref,
    after_ref,
):
    experts, capacity, _ = sent_ref.shape
    target_a, target_b = targets_row(choice_ref[...], capacity)
    tokens = target_a.shape[1]
    slots = experts * capacity

    def one_hot(condition):
        one = jnp.ones(condition.shape, F32)
        return jnp.where(condition, one, jnp.zeros_like(one)).astype(BF16)

    slot = sublanes((slots, tokens))
    place = one_hot((slot == target_a) | (slot == target_b))
    weight = weight_ref[...]
    for k, target in enumerate((target_a, target_b)):
        column = column_of(target)
        for half in range(2):
            order = slot_of((tokens, slots // 2), 1, capacity, half)
            pick_ref[2 * k + half] = one_hot(order == column)
        weight_out_ref[k] = jnp.broadcast_to(
            column_of(weight[k : k + 1, :]), weight_out_ref.shape[1:]
        )
    peers, rows, _ = arrived_ref.shape
    width = whole_ref.shape[1]
    lane = lanes((rows, 128))
    quarters = []
    for q in range(4):
        tiles = []
        for m in range(peers // 4):
            tile = None
            for k in range(4):
                piece = lane_roll(arrived_ref[4 * m + k].astype(F32), (k - q) * 32)
                tile = piece if tile is None else jnp.where(lane // 32 == k, piece, tile)
            tiles.append(tile)
        quarters.append(jnp.concatenate(tiles, axis=1))
    mixer = jnp.concatenate(quarters, axis=0).astype(BF16)
    mixed = dot(mixer, w_out_ref[...]).astype(BF16).astype(F32)
    after = (whole_ref[...].astype(F32) + mixed).astype(BF16).astype(F32)
    after_ref[...] = after
    scale = lax.rsqrt(jnp.sum(after * after, axis=1, keepdims=True) / width + 1e-06)
    part = sent_ref.shape[2]
    rank = lax.axis_index(TP)
    start = pl.multiple_of(lax.axis_index(NEAR) * part, 128)
    gain = gain_ref[:, pl.ds(start, part)]
    normed = (after_ref[:, pl.ds(start, part)] * scale * gain).astype(BF16)
    sent_ref[...] = dot(place, normed).astype(BF16).reshape(experts, capacity, part)
    own = after_ref[:, pl.ds(pl.multiple_of(rank // 2 * 128, 128), 128)]
    odd = jnp.broadcast_to(rank % 2, own.shape) == 1
    own_ref[...] = jnp.where(odd, lane_roll(own, 64), own)


def expert_kernel(
    piece_ref,
    gate_ref,
    up_ref,
    down_ref,
    state_re_ref,
    state_im_ref,
    parts_ref,
    out_re_ref,
    out_im_ref,
    sems,
):
    copies = [
        pltpu.make_async_copy(state_re_ref, out_re_ref, sems.at[0]),
        pltpu.make_async_copy(state_im_ref, out_im_ref, sems.at[1]),
    ]
    for copy in copies:
        copy.start()
    pieces, _, share = piece_ref.shape
    count, _, part = parts_ref.shape
    gate = upper = None
    for k in range(pieces):
        piece = piece_ref[k]
        g = dot(piece, gate_ref[k * share : (k + 1) * share, :])
        u = dot(piece, up_ref[k * share : (k + 1) * share, :])
        gate = g if gate is None else gate + g
        upper = u if upper is None else upper + u
    hidden = (jax.nn.silu(gate) * upper).astype(BF16)
    rows = hidden.shape[0]
    low = lanes((rows, 128)) < 64
    block = 64 * count
    for m in range(part // 128):
        value = dot(hidden, down_ref[:, 2 * m * block : (2 * m + 2) * block])
        for k in range(count):
            a = value[:, k // 2 * 128 : k // 2 * 128 + 128]
            b = value[:, block + k // 2 * 128 : block + k // 2 * 128 + 128]
            if k % 2:
                joined = jnp.where(low, lane_roll(a, 64), b)
            else:
                joined = jnp.where(low, a, lane_roll(b, 64))
            parts_ref[k, :, m * 128 : (m + 1) * 128] = joined.astype(BF16)
    for copy in copies:
        copy.wait()


def sum_kernel(capacity, arrived_ref, out_ref):
    total = arrived_ref[0].astype(F32)
    for k in range(1, arrived_ref.shape[0]):
        total = total + arrived_ref[k].astype(F32)
    total = total.astype(BF16)
    slots = total.shape[0]
    halves = []
    for half in range(2):
        order = slot_of((slots // 2, slots), 0, capacity, half)
        one = jnp.ones(order.shape, F32)
        pick = jnp.where(order == lanes(order.shape), one, jnp.zeros_like(one)).astype(BF16)
        halves.append(dot(pick, total))
    first, second = halves
    experts, rows, short, _ = out_ref.shape
    low = lanes((slots // 2, 128)) < 64
    for m in range(rows // 2):
        a = first[:, m * 128 : (m + 1) * 128]
        b = second[:, m * 128 : (m + 1) * 128]
        even = jnp.where(low, a, lane_roll(b, 64)).astype(BF16)
        odd = jnp.where(low, lane_roll(a, 64), b).astype(BF16)
        out_ref[:, 2 * m] = even.reshape(experts, short, 128)
        out_ref[:, 2 * m + 1] = odd.reshape(experts, short, 128)


def combine_kernel(returned_ref, pick_ref, weight_ref, own_ref, out_ref):
    experts, rows, short, _ = returned_ref.shape
    returned = returned_ref[:, 0].astype(F32)
    for k in range(1, rows):
        returned = returned + returned_ref[:, k].astype(F32)
    returned = returned.reshape(experts * short, 128).astype(BF16)
    total = own_ref[:, :64]
    for k in range(2):
        picked = dot(pick_ref[2 * k], returned)[:, :64] + dot(pick_ref[2 * k + 1], returned)[:, 64:]
        total = total + picked * weight_ref[k]
    out_ref[...] = total.astype(BF16)


def body(
    tokens,
    gain_mix,
    w_in,
    decay_rate,
    frequency,
    log_step,
    input_real,
    input_imag,
    readout_real,
    readout_imaginary,
    passthrough_scale,
    state_real,
    state_imag,
    w_out,
    gain_ffn,
    expert_choice,
    expert_weight,
    w_gate,
    w_up,
    w_down,
):
    near, far, experts = lax.axis_size(NEAR), lax.axis_size("yh"), lax.axis_size("ep")
    tp_count = near * far
    rows, local_width = tokens.shape
    full_width = local_width * tp_count
    share = full_width // near
    capacity = 2 * rows * expert_choice.shape[1] // experts
    slots = experts * capacity
    groups, state = decay_rate.shape
    channels = passthrough_scale.shape[0]
    sds = jax.ShapeDtypeStruct

    copies = call(spread_kernel, sds((tp_count, rows // 2, 128), BF16), tokens)
    arrived = exchange(copies, TP)
    whole, next_re, next_im, mixer = call(
        mixer_kernel,
        (
            sds((rows, full_width), BF16),
            sds(state_real.shape, F32),
            sds(state_real.shape, F32),
            sds((tp_count, rows // 4, 128), BF16),
        ),
        arrived,
        gain_mix.reshape(1, full_width),
        w_in.T,
        decay_rate,
        frequency,
        log_step,
        jnp.swapaxes(input_real, 1, 2),
        jnp.swapaxes(input_imag, 1, 2),
        readout_real,
        readout_imaginary,
        passthrough_scale.reshape(1, channels),
        state_real,
        state_imag,
        smem=(5,),
    )
    arrived = exchange(mixer, TP)
    sent, own, picks, weights = call(
        dispatch_kernel,
        (
            sds((experts, capacity, share), BF16),
            sds((rows, 128), F32),
            sds((4, rows, slots // 2), BF16),
            sds((2, rows, local_width), F32),
        ),
        arrived,
        whole,
        w_out,
        gain_ffn.reshape(1, full_width),
        expert_choice.T,
        expert_weight.T,
        scratch=(pltpu.VMEM((rows, full_width), F32),),
    )
    arrived = exchange(sent, "ep").reshape(slots, share)
    pieces = exchange(jnp.broadcast_to(arrived, (near, slots, share)), NEAR)
    parts, next_re, next_im = call(
        expert_kernel,
        (
            sds((near, slots, far * local_width), BF16),
            sds(state_real.shape, F32),
            sds(state_real.shape, F32),
        ),
        pieces,
        w_gate[0],
        w_up[0],
        w_down[0],
        next_re,
        next_im,
        hbm_outs=(1, 2),
        scratch=(pltpu.SemaphoreType.DMA((2,)),),
    )
    arrived = exchange(parts, NEAR)
    short = capacity // 2
    results = call(
        functools.partial(sum_kernel, capacity), sds((experts, far, short, 128), BF16), arrived
    )
    returned = exchange(results.reshape(experts * far, short, 128), ("ep", "yh"))
    returned = returned.reshape(experts, far, short, 128)
    layer_out = call(
        combine_kernel, sds((rows, local_width), BF16), returned, picks, weights, own
    )
    return (layer_out, next_re, next_im)


def solution(mesh):
    tp_count = mesh.shape["tp"]
    devices = mesh.devices.reshape(
        mesh.shape["ep"], tp_count // (Y_LOW * X_COUNT), Y_LOW, X_COUNT
    )
    tp = TP
    return jax.shard_map(
        body,
        mesh=Mesh(devices, ("ep", *TP)),
        in_specs=(
            P("ep", tp),
            P(),
            P(None, tp),
            P(tp, None),
            P(tp, None),
            P(tp),
            P(tp, None, None),
            P(tp, None, None),
            P(tp, None, None),
            P(tp, None, None),
            P(tp),
            P("ep", tp, None),
            P("ep", tp, None),
            P(),
            P(),
            P("ep", None),
            P("ep", None),
            P("ep", None, tp),
            P("ep", None, tp),
            P("ep", tp, None),
        ),
        out_specs=(P("ep", tp), P("ep", tp, None), P("ep", tp, None)),
        check_vma=False,
    )
```

```python
import functools

import jax
import jax.numpy as jnp
from jax import lax
from jax.experimental import pallas as pl
from jax.experimental.pallas import tpu as pltpu
from jax.sharding import Mesh
from jax.sharding import PartitionSpec as P

F32 = jnp.float32
BF16 = jnp.bfloat16
X_COUNT = 4
Y_LOW = 2
TP = ("yh", "yl", "x")
NEAR = ("yl", "x")
FLOPS = 4_000_000_000
VMEM_LIMIT = 16 * 1024 * 1024


def exchange(parts, axis):
    return lax.all_to_all(parts, axis, split_axis=0, concat_axis=0, tiled=True)


def call(kernel, out_shape, *args, smem=(), hbm_outs=(), scratch=(), flops=FLOPS):
    specs = [
        pl.BlockSpec(
            memory_space=pltpu.SMEM if i in smem else pltpu.VMEM
        )
        for i in range(len(args))
    ]
    if isinstance(out_shape, tuple):
        outs = tuple(
            pl.BlockSpec(memory_space=pltpu.HBM if i in hbm_outs else pltpu.VMEM)
            for i in range(len(out_shape))
        )
    else:
        outs = pl.BlockSpec(memory_space=pltpu.VMEM)
    return pl.pallas_call(
        kernel,
        out_shape=out_shape,
        in_specs=specs,
        out_specs=outs,
        scratch_shapes=list(scratch),
        cost_estimate=pl.CostEstimate(flops=flops, bytes_accessed=0, transcendentals=0),
        compiler_params=pltpu.CompilerParams(vmem_limit_bytes=VMEM_LIMIT),
    )(*args)


def lanes(shape):
    return lax.broadcasted_iota(jnp.int32, shape, len(shape) - 1)


def sublanes(shape):
    return lax.broadcasted_iota(jnp.int32, shape, len(shape) - 2)


def lane_roll(value, amount):
    return pltpu.roll(value, amount % value.shape[-1], value.ndim - 1)


def dot(a, b):
    return jnp.dot(a, b, preferred_element_type=F32)


def dot_nt(a, b):
    return lax.dot_general(a, b, (((1,), (1,)), ((), ())), preferred_element_type=F32)


def column_of(row):
    n = row.shape[-1]
    eye = sublanes((n, n)) == lanes((n, n))
    return jnp.sum(jnp.where(eye, jnp.broadcast_to(row, (n, n)), jnp.zeros((n, n), row.dtype)), axis=1, keepdims=True)


def spread_kernel(tokens_ref, out_ref):
    half = tokens_ref.shape[0] // 2
    values = tokens_ref[...].astype(F32)
    pair = jnp.concatenate([values[:half], values[half:]], axis=1).astype(BF16)
    for t in range(out_ref.shape[0]):
        out_ref[t] = pair


def targets_row(choice, capacity):
    n = choice.shape[1]
    first, second = choice[0:1, :], choice[1:2, :]
    first_col, second_col = column_of(first), column_of(second)
    earlier = sublanes((n, n)) < lanes((n, n))
    one = jnp.ones((n, n), jnp.int32)
    none = jnp.zeros((n, n), jnp.int32)
    slot_a = jnp.sum(jnp.where((first_col == first) & earlier, one, none), axis=0, keepdims=True)
    slot_b = jnp.sum(
        jnp.where(first_col == second, one, none)
        + jnp.where((second_col == second) & earlier, one, none),
        axis=0,
        keepdims=True,
    )
    return first * capacity + slot_a, second * capacity + slot_b


def slot_of(shape, axis, capacity, half):
    index = lax.broadcasted_iota(jnp.int32, shape, axis)
    short = capacity // 2
    return index // short * capacity + half * short + index % short


def mixer_kernel(
    arrived_ref,
    gain_ref,
    w_in_ref,
    decay_ref,
    freq_ref,
    log_step_ref,
    in_re_ref,
    in_im_ref,
    out_re_ref,
    out_im_ref,
    pass_ref,
    state_re_ref,
    state_im_ref,
    whole_ref,
    next_re_ref,
    next_im_ref,
    mixer_ref,
):
    groups, state = decay_ref.shape
    step = jnp.concatenate(
        [jnp.exp(jnp.full((1, state), log_step_ref[g], F32)) for g in range(groups)], axis=1
    )
    decay = jnp.concatenate([decay_ref[g : g + 1, :] for g in range(groups)], axis=1)
    freq = jnp.concatenate([freq_ref[g : g + 1, :] for g in range(groups)], axis=1)
    lam_re = -decay
    magnitude = jnp.exp(lam_re * step)
    abar_re = magnitude * jnp.cos(freq * step)
    abar_im = magnitude * jnp.sin(freq * step)
    denom = lam_re * lam_re + freq * freq
    numer = abar_re - 1.0
    factor_re = (numer * lam_re + abar_im * freq) / denom
    factor_im = (abar_im * lam_re - numer * freq) / denom

    def blocks(ref):
        rows = []
        for g in range(groups):
            zero = jnp.zeros_like(ref[g])
            rows.append(jnp.concatenate([ref[g] if k == g else zero for k in range(groups)], axis=1))
        return jnp.concatenate(rows, axis=0)

    in_re, in_im = blocks(in_re_ref), blocks(in_im_ref)
    bbar_re = factor_re * in_re - factor_im * in_im
    bbar_im = factor_re * in_im + factor_im * in_re

    peers, half, _ = arrived_ref.shape
    width = peers * 64
    low = lanes((half, 128)) < 64
    tops, bottoms = [], []
    for m in range(peers // 2):
        a = arrived_ref[2 * m].astype(F32)
        b = arrived_ref[2 * m + 1].astype(F32)
        tops.append(jnp.where(low, a, lane_roll(b, 64)))
        bottoms.append(jnp.where(low, lane_roll(a, 64), b))
    whole = jnp.concatenate(
        [jnp.concatenate(tops, axis=1), jnp.concatenate(bottoms, axis=1)], axis=0
    )
    whole_ref[...] = whole.astype(BF16)
    scale = lax.rsqrt(jnp.sum(whole * whole, axis=1, keepdims=True) / width + 1e-06)
    normed = (whole * scale * gain_ref[...]).astype(BF16)
    drive = dot_nt(normed, w_in_ref[...]).astype(BF16).astype(F32)

    state_re = jnp.concatenate([state_re_ref[:, g, :] for g in range(groups)], axis=1)
    state_im = jnp.concatenate([state_im_ref[:, g, :] for g in range(groups)], axis=1)
    next_re = abar_re * state_re - abar_im * state_im + dot(drive, bbar_re)
    next_im = abar_re * state_im + abar_im * state_re + dot(drive, bbar_im)
    readout = (
        dot_nt(next_re, blocks(out_re_ref))
        - dot_nt(next_im, blocks(out_im_ref))
        + pass_ref[...] * drive
    )
    mixer = jax.nn.gelu(readout)
    rows = mixer.shape[0] // 4
    packed = jnp.concatenate([mixer[q * rows : (q + 1) * rows] for q in range(4)], axis=1).astype(BF16)
    for t in range(mixer_ref.shape[0]):
        mixer_ref[t] = packed
    state = state_re_ref.shape[2]
    for g in range(groups):
        next_re_ref[:, g, :] = next_re[:, g * state : (g + 1) * state]
        next_im_ref[:, g, :] = next_im[:, g * state : (g + 1) * state]


def dispatch_kernel(
    arrived_ref,
    whole_ref,
    w_out_ref,
    gain_ref,
    choice_ref,
    weight_ref,
    sent_ref,
    own_ref,
    pick_ref,
    weight_out_ref,
    after_ref,
):
    experts, capacity, _ = sent_ref.shape
    target_a, target_b = targets_row(choice_ref[...], capacity)
    tokens = target_a.shape[1]
    slots = experts * capacity

    def one_hot(condition):
        one = jnp.ones(condition.shape, F32)
        return jnp.where(condition, one, jnp.zeros_like(one)).astype(BF16)

    slot = sublanes((slots, tokens))
    place = one_hot((slot == target_a) | (slot == target_b))
    weight = weight_ref[...]
    for k, target in enumerate((target_a, target_b)):
        column = column_of(target)
        for half in range(2):
            order = slot_of((tokens, slots // 2), 1, capacity, half)
            pick_ref[2 * k + half] = one_hot(order == column)
        weight_out_ref[k] = jnp.broadcast_to(
            column_of(weight[k : k + 1, :]), weight_out_ref.shape[1:]
        )
    peers, rows, _ = arrived_ref.shape
    width = whole_ref.shape[1]
    lane = lanes((rows, 128))
    quarters = []
    for q in range(4):
        tiles = []
        for m in range(peers // 4):
            tile = None
            for k in range(4):
                piece = lane_roll(arrived_ref[4 * m + k].astype(F32), (k - q) * 32)
                tile = piece if tile is None else jnp.where(lane // 32 == k, piece, tile)
            tiles.append(tile)
        quarters.append(jnp.concatenate(tiles, axis=1))
    mixer = jnp.concatenate(quarters, axis=0).astype(BF16)
    mixed = dot(mixer, w_out_ref[...]).astype(BF16).astype(F32)
    after = (whole_ref[...].astype(F32) + mixed).astype(BF16).astype(F32)
    after_ref[...] = after
    scale = lax.rsqrt(jnp.sum(after * after, axis=1, keepdims=True) / width + 1e-06)
    part = sent_ref.shape[2]
    rank = lax.axis_index(TP)
    start = pl.multiple_of(lax.axis_index(NEAR) * part, 128)
    gain = gain_ref[:, pl.ds(start, part)]
    normed = (after_ref[:, pl.ds(start, part)] * scale * gain).astype(BF16)
    sent_ref[...] = dot(place, normed).astype(BF16).reshape(experts, capacity, part)
    own = after_ref[:, pl.ds(pl.multiple_of(rank // 2 * 128, 128), 128)]
    odd = jnp.broadcast_to(rank % 2, own.shape) == 1
    own_ref[...] = jnp.where(odd, lane_roll(own, 64), own)


def expert_kernel(
    piece_ref,
    gate_ref,
    up_ref,
    down_ref,
    state_re_ref,
    state_im_ref,
    parts_ref,
    out_re_ref,
    out_im_ref,
    sems,
):
    copies = [
        pltpu.make_async_copy(state_re_ref, out_re_ref, sems.at[0]),
        pltpu.make_async_copy(state_im_ref, out_im_ref, sems.at[1]),
    ]
    for copy in copies:
        copy.start()
    pieces, _, share = piece_ref.shape
    gate = upper = None
    for k in range(pieces):
        piece = piece_ref[k]
        g = dot(piece, gate_ref[k * share : (k + 1) * share, :])
        u = dot(piece, up_ref[k * share : (k + 1) * share, :])
        gate = g if gate is None else gate + g
        upper = u if upper is None else upper + u
    hidden = (jax.nn.silu(gate) * upper).astype(BF16)
    block = 8 * 64
    for m in range(parts_ref.shape[0] * 64 // block):
        value = dot(hidden, down_ref[:, m * block : (m + 1) * block]).T
        for k in range(8):
            parts_ref[8 * m + k] = value[k * 64 : (k + 1) * 64, :].astype(BF16)
    for copy in copies:
        copy.wait()


def sum_kernel(capacity, arrived_ref, out_ref):
    total = arrived_ref[0].astype(F32)
    for k in range(1, arrived_ref.shape[0]):
        total = total + arrived_ref[k].astype(F32)
    total = total.astype(BF16)
    slots = total.shape[1]
    halves = []
    for half in range(2):
        order = slot_of((slots // 2, slots), 0, capacity, half)
        one = jnp.ones(order.shape, F32)
        pick = jnp.where(order == lanes(order.shape), one, jnp.zeros_like(one)).astype(BF16)
        halves.append(dot_nt(pick, total))
    out_ref[...] = jnp.concatenate(halves, axis=1).astype(BF16).reshape(out_ref.shape)


def combine_kernel(returned_ref, pick_ref, weight_ref, own_ref, out_ref):
    returned = returned_ref[...]
    returned = returned.reshape(returned.shape[0] * returned.shape[1], 128)
    total = own_ref[:, :64]
    for k in range(2):
        picked = dot(pick_ref[2 * k], returned)[:, :64] + dot(pick_ref[2 * k + 1], returned)[:, 64:]
        total = total + picked * weight_ref[k]
    out_ref[...] = total.astype(BF16)


def body(
    tokens,
    gain_mix,
    w_in,
    decay_rate,
    frequency,
    log_step,
    input_real,
    input_imag,
    readout_real,
    readout_imaginary,
    passthrough_scale,
    state_real,
    state_imag,
    w_out,
    gain_ffn,
    expert_choice,
    expert_weight,
    w_gate,
    w_up,
    w_down,
):
    near, far, experts = lax.axis_size(NEAR), lax.axis_size("yh"), lax.axis_size("ep")
    tp_count = near * far
    rows, local_width = tokens.shape
    full_width = local_width * tp_count
    share = full_width // near
    capacity = 2 * rows * expert_choice.shape[1] // experts
    slots = experts * capacity
    groups, state = decay_rate.shape
    channels = passthrough_scale.shape[0]
    sds = jax.ShapeDtypeStruct

    copies = call(spread_kernel, sds((tp_count, rows // 2, 128), BF16), tokens)
    arrived = exchange(copies, TP)
    whole, next_re, next_im, mixer = call(
        mixer_kernel,
        (
            sds((rows, full_width), BF16),
            sds(state_real.shape, F32),
            sds(state_real.shape, F32),
            sds((tp_count, rows // 4, 128), BF16),
        ),
        arrived,
        gain_mix.reshape(1, full_width),
        w_in.T,
        decay_rate,
        frequency,
        log_step,
        jnp.swapaxes(input_real, 1, 2),
        jnp.swapaxes(input_imag, 1, 2),
        readout_real,
        readout_imaginary,
        passthrough_scale.reshape(1, channels),
        state_real,
        state_imag,
        smem=(5,),
    )
    arrived = exchange(mixer, TP)
    sent, own, picks, weights = call(
        dispatch_kernel,
        (
            sds((experts, capacity, share), BF16),
            sds((rows, 128), F32),
            sds((4, rows, slots // 2), BF16),
            sds((2, rows, local_width), F32),
        ),
        arrived,
        whole,
        w_out,
        gain_ffn.reshape(1, full_width),
        expert_choice.T,
        expert_weight.T,
        scratch=(pltpu.VMEM((rows, full_width), F32),),
    )
    arrived = exchange(sent, "ep").reshape(slots, share)
    pieces = exchange(jnp.broadcast_to(arrived, (near, slots, share)), NEAR)
    parts, next_re, next_im = call(
        expert_kernel,
        (
            sds((tp_count, local_width, slots), BF16),
            sds(state_real.shape, F32),
            sds(state_real.shape, F32),
        ),
        pieces,
        w_gate[0],
        w_up[0],
        w_down[0],
        next_re,
        next_im,
        hbm_outs=(1, 2),
        scratch=(pltpu.SemaphoreType.DMA((2,)),),
    )
    arrived = exchange(parts, TP)
    results = call(
        functools.partial(sum_kernel, capacity), sds((experts, capacity // 2, 128), BF16), arrived
    )
    returned = exchange(results, "ep")
    layer_out = call(
        combine_kernel, sds((rows, local_width), BF16), returned, picks, weights, own
    )
    return (layer_out, next_re, next_im)


def solution(mesh):
    tp_count = mesh.shape["tp"]
    devices = mesh.devices.reshape(
        mesh.shape["ep"], tp_count // (Y_LOW * X_COUNT), Y_LOW, X_COUNT
    )
    tp = TP
    return jax.shard_map(
        body,
        mesh=Mesh(devices, ("ep", *TP)),
        in_specs=(
            P("ep", tp),
            P(),
            P(None, tp),
            P(tp, None),
            P(tp, None),
            P(tp),
            P(tp, None, None),
            P(tp, None, None),
            P(tp, None, None),
            P(tp, None, None),
            P(tp),
            P("ep", tp, None),
            P("ep", tp, None),
            P(),
            P(),
            P("ep", None),
            P("ep", None),
            P("ep", None, tp),
            P("ep", None, tp),
            P("ep", tp, None),
        ),
        out_specs=(P("ep", tp), P("ep", tp, None), P("ep", tp, None)),
        check_vma=False,
    )
```
